128 devices in a mesh: sp: 16 (over z, x), fs: 4 (over y), tp: 2 (over core).
Axes of the slice: x: 4, y: 4, z: 4, core: 2. Of those that a mesh axis runs over, the one named last changes fastest.
Arguments:
- stream: bfloat16 [4, 16384, 2048], P('fs', 'sp', 'tp'), parts along dimension 0, may hold values from -6 to 6
- w_pool_in: bfloat16 [2048, 1024], P(None, 'tp'), may hold values from -0.125 to 0.125
- w_query: bfloat16 [2048, 1024], P(None, 'tp'), may hold values from -0.125 to 0.125
- w_forget: bfloat16 [2048, 1024], P(None, 'tp'), may hold values from -0.125 to 0.125
- w_value: bfloat16 [2048, 1024], P(None, 'tp'), may hold values from -0.125 to 0.125
- w_outgate: bfloat16 [2048, 1024], P(None, 'tp'), may hold values from -0.125 to 0.125
- pool_mix: bfloat16 [4, 256, 256], P('tp'), may hold values from -0.375 to 0.375
- pool_scale: float32 [1024], P('tp'), may hold values from 0.1 to 1.9
- lower_bound: float32 [1024], P('tp'), may hold values from 0.9 to 1
- extra_decay: float32 [16384, 8], P('sp', 'tp'), may hold values from -0.7 to 0
- rec_gain: float32 [128], replicated, may hold values from 0.1 to 1.9
- w_out_pool: bfloat16 [1024, 2048], P('tp'), may hold values from -0.125 to 0.125
- w_out_rec: bfloat16 [1024, 2048], P('tp'), may hold values from -0.125 to 0.125
- norm_gain: float32 [2048], P('tp'), may hold values from 0.1 to 1.9
- norm_bias: float32 [2048], P('tp'), may hold values from -3 to 3
Outputs:
- layer_out: bfloat16 [4, 16384, 2048], P('fs', 'sp', 'tp'), parts along dimension 0
The draws below stay inside these ranges and needn't reach their ends.
There are 4 independent parts, one for each index of `fs`. The reference program is written for one: setup_inputs(seed, part) draws one part's arguments, and reference() takes and returns one part's arrays. A program takes and returns all parts, laid end to end along the dimension named above; an argument that names none is the same for every part. Nothing has to cross between parts.
All inputs are finite; a program needn't handle non-finite values.
Results may differ from the reference program's by a relative error of at most 0.0085.
Values may be sent and summed in bfloat16 or wider, within the bound.
A program may use at most 128 MiB of HBM per device.

```python
import math
import jax
import jax.numpy as jnp
from jax import lax

D = 2048
POOL_W = 1024
REC_W = 1024
DK = 128
WMAX = 16
BLOCK_ROWS = 128
TOK_DEV = 1024
GROUP_CH = 256
HEADS = 8
SEQ = 16384


def draw_lower_bound(key, part):
    key_order = jax.random.fold_in(key, 11)
    key_fast = jax.random.fold_in(key, 12)
    key_slow = jax.random.fold_in(key, 13)
    order = jax.random.permutation(key_order, HEADS)
    chosen = order < HEADS // 2
    fast_gap = jnp.exp(jax.random.uniform(key_fast, (HEADS, DK), jnp.float32, math.log(0.03), math.log(0.06)))
    slow_gap = jnp.exp(jax.random.uniform(key_slow, (HEADS, DK), jnp.float32, math.log(0.16 / SEQ), math.log(0.8 / SEQ)))
    gaps = jnp.where(chosen[:, None], fast_gap, slow_gap)
    return (1.0 - gaps).reshape(REC_W).astype(jnp.float32)


def draw_extra_decay(key, part):
    key_base = jax.random.fold_in(key, 21)
    key_where = jax.random.fold_in(key, 22)
    key_drop = jax.random.fold_in(key, 23)
    blocks = SEQ // TOK_DEV
    base = jnp.exp(jax.random.uniform(key_base, (blocks,), jnp.float32, math.log(0.04 / SEQ), math.log(0.2 / SEQ)))
    base_rows = jnp.repeat(base, TOK_DEV)
    places = jax.random.randint(key_where, (2,), 0, SEQ)
    marked = jnp.any(jnp.arange(SEQ)[:, None] == places[None, :], axis=1)
    drops = jax.random.uniform(key_drop, (SEQ, HEADS), jnp.float32, 0.22, 0.69)
    total = base_rows[:, None] + jnp.where(marked[:, None], drops, jnp.float32(0.0))
    return (-total).astype(jnp.float32)


def shard_levels(rng, shape, split, least, largest):
    gain = 1.0
    for axis_at, parts in split:
        draws = jax.random.uniform(jax.random.fold_in(jax.random.fold_in(rng, 6), axis_at), (parts,), jnp.float32, least / len(split), largest / len(split))
        gain = gain * jnp.repeat(jnp.exp(draws), shape[axis_at] // parts).reshape((-1,) + (1,) * (len(shape) - 1 - axis_at))
    return gain


def normal_values(key, dims, width, bound, shards=(), dtype=jnp.bfloat16):
    factor_of = shard_levels(key, dims, shards, -0.22, 0.18) if shards else 1.0
    result = jax.random.normal(key, dims, jnp.float32) * width * factor_of
    return jnp.minimum(jnp.maximum(result, -bound), bound).astype(dtype)


def setup_inputs(seed: int = 0, part: int = 0) -> dict:
    key_list = jax.random.split(jax.random.key(seed), 16)
    own_keys = jax.random.split(jax.random.fold_in(key_list[15], part), 16)
    return {
        "stream": normal_values(own_keys[0], (1, SEQ, D), 1.0, 6.0, ((1, 16), (2, 2))),
        "w_pool_in": normal_values(key_list[1], (D, POOL_W), D ** -0.5, 0.125, ((1, 2),)),
        "w_query": normal_values(key_list[2], (D, REC_W), D ** -0.5, 0.125, ((1, 2),)),
        "w_forget": normal_values(key_list[3], (D, REC_W), D ** -0.5, 0.125, ((1, 2),)),
        "w_value": normal_values(key_list[4], (D, REC_W), D ** -0.5, 0.125, ((1, 2),)),
        "w_outgate": normal_values(key_list[5], (D, REC_W), D ** -0.5, 0.125, ((1, 2),)),
        "pool_mix": normal_values(key_list[6], (4, GROUP_CH, GROUP_CH), GROUP_CH ** -0.5, 0.375, ((0, 2),)),
        "pool_scale": jnp.clip(1.0 + 0.18 * jax.random.normal(key_list[7], (POOL_W,), jnp.float32), 0.1, 1.9),
        "lower_bound": draw_lower_bound(jax.random.fold_in(key_list[15], 71), part),
        "extra_decay": draw_extra_decay(jax.random.fold_in(key_list[15], 71), part),
        "rec_gain": jnp.clip(1.0 + 0.18 * jax.random.normal(key_list[10], (DK,), jnp.float32), 0.1, 1.9),
        "w_out_pool": normal_values(key_list[11], (POOL_W, D), (POOL_W + REC_W) ** -0.5, 0.125, ((0, 2),)),
        "w_out_rec": normal_values(key_list[12], (REC_W, D), (POOL_W + REC_W) ** -0.5, 0.125, ((0, 2),)),
        "norm_gain": jnp.clip(1.0 + 0.18 * jax.random.normal(key_list[13], (D,), jnp.float32), 0.1, 1.9),
        "norm_bias": normal_values(key_list[14], (D,), 0.5, 3.0, ((0, 2),), jnp.float32),
    }


ALPHA = 2.0 ** 0.25
EPS_RMS = 1e-06
EPS_NORM = 1e-05
HIGHEST = lax.Precision.HIGHEST

def pool_branch(pooled, pool_mix, pool_scale):
    length = pooled.shape[0]
    data = pooled.astype(jnp.float32)
    padded = jnp.pad(data, ((WMAX - 1, 0), (0, 0)))
    group_id = jnp.arange(POOL_W).astype(jnp.int32) // GROUP_CH
    window_len = jnp.left_shift(jnp.ones_like(group_id), group_id + 1)
    window_sum = jnp.zeros((length, POOL_W), jnp.float32)
    for lag_rows in range(WMAX):
        lagged = padded[WMAX - 1 - lag_rows:WMAX - 1 - lag_rows + length]
        window_sum = window_sum + jnp.where(lag_rows < window_len[None, :], lagged, jnp.float32(0.0))
    position = jnp.arange(1, length + 1).astype(jnp.float32)
    counts = jnp.minimum(position[:, None], window_len.astype(jnp.float32)[None, :])
    pool_diff = (window_sum / counts - data).astype(jnp.bfloat16)
    grouped = pool_diff.reshape(length, 4, GROUP_CH).astype(jnp.float32)
    mixed = jnp.einsum('tgc,gcd->tgd', grouped, pool_mix.astype(jnp.float32))
    return (mixed.reshape(length, POOL_W) * pool_scale).astype(jnp.bfloat16)

def recurrent_branch(queries, forget_in, value_in, gate_in, lower_bound, extra_decay, rec_gain):
    length = queries.shape[0]
    blocks = length // BLOCK_ROWS
    forget = lower_bound + (1.0 - lower_bound) * jax.nn.sigmoid(forget_in.astype(jnp.float32))
    log_keep = jnp.log(forget).reshape(length, HEADS, DK) + extra_decay[:, :, None]
    weight_in = (1.0 - forget).reshape(length, HEADS, DK)
    gated_query = jax.nn.silu(queries.astype(jnp.float32)).reshape(length, HEADS, DK)
    values = value_in.reshape(length, HEADS, DK)

    def to_blocks(arr):
        return arr.reshape(blocks, BLOCK_ROWS, HEADS, DK)
    lower_mask = jnp.tril(jnp.ones((BLOCK_ROWS, BLOCK_ROWS), jnp.float32))

    def block_step(state, inputs):
        query_blk, keep_blk, input_blk, value_blk = inputs
        value_wide = value_blk.astype(jnp.float32)
        log_total = jnp.cumsum(keep_blk, axis=0)
        query_up = query_blk * jnp.exp(log_total)
        input_down = input_blk * jnp.exp(-log_total)
        scores = jnp.einsum('thd,shd->hts', query_up, input_down, precision=HIGHEST) * lower_mask[None]
        scores = scores.astype(jnp.bfloat16).astype(jnp.float32)
        inside = jnp.einsum('hts,she->the', scores, value_wide, precision=HIGHEST)
        carried = jnp.einsum('thd,hde->the', query_up, state, precision=HIGHEST)
        log_end = log_total[-1]
        in_weight = (input_blk * jnp.exp(log_end[None] - log_total)).astype(jnp.bfloat16).astype(jnp.float32)
        new_state = jnp.exp(log_end)[:, :, None] * state + jnp.einsum('shd,she->hde', in_weight, value_wide, precision=HIGHEST)
        return (new_state, inside + carried)
    start_state = jnp.zeros((HEADS, DK, DK), jnp.float32)
    _, outputs = lax.scan(block_step, start_state, (to_blocks(gated_query), to_blocks(log_keep), to_blocks(weight_in), to_blocks(values)))
    rec_raw = outputs.reshape(length, HEADS, DK)
    rec_norm = rec_raw * lax.rsqrt(lax.optimization_barrier(jnp.mean(rec_raw * rec_raw, axis=-1, keepdims=True)) + EPS_RMS) * rec_gain
    gated = rec_norm * jax.nn.silu(gate_in.astype(jnp.float32)).reshape(length, HEADS, DK)
    return gated.reshape(length, REC_W).astype(jnp.bfloat16)

def reference(stream, w_pool_in, w_query, w_forget, w_value, w_outgate, pool_mix, pool_scale, lower_bound, extra_decay, rec_gain, w_out_pool, w_out_rec, norm_gain, norm_bias):
    features = stream[0]

    def project(weight):
        return jnp.dot(features, weight, preferred_element_type=jnp.float32).astype(jnp.bfloat16)
    pooled = project(w_pool_in)
    queries = project(w_query)
    forget_in = project(w_forget)
    value_in = project(w_value)
    gate_in = project(w_outgate)
    pool_out = pool_branch(pooled, pool_mix, pool_scale)
    rec_out = recurrent_branch(queries, forget_in, value_in, gate_in, lower_bound, extra_decay, rec_gain)
    mix = jnp.dot(pool_out, w_out_pool, preferred_element_type=jnp.float32) + jnp.dot(rec_out, w_out_rec, preferred_element_type=jnp.float32)
    resid = ALPHA * features.astype(jnp.float32) + mix
    row_mean = lax.optimization_barrier(jnp.mean(resid, axis=-1, keepdims=True))
    row_var = lax.optimization_barrier(jnp.mean((resid - row_mean) * (resid - row_mean), axis=-1, keepdims=True))
    normed = (resid - row_mean) * lax.rsqrt(row_var + EPS_NORM) * norm_gain + norm_bias
    return normed.astype(jnp.bfloat16)[None]
```

```python
import functools

import jax
import jax.numpy as jnp
from jax import lax
from jax.experimental import pallas as pl
from jax.experimental.pallas import tpu as pltpu
from jax.sharding import Mesh
from jax.sharding import PartitionSpec as P

BF16 = jnp.bfloat16
F32 = jnp.float32
MESH = pl.DeviceIdType.MESH

ALPHA = 2.0**0.25
EPS_RMS = 1e-06
EPS_NORM = 1e-05

T = 1024
H = 1024
C = 512
DK = 128
NH = C // DK
B = 128
NB = T // B
R = 256
NT = T // R
NX = 4
MSG = DK + 16


def dot(a, b):
    return jnp.dot(a, b, preferred_element_type=F32)


def dot_tn(a, b):
    return lax.dot_general(a, b, (((0,), (0,)), ((), ())), preferred_element_type=F32)


def dot_nt(a, b):
    return lax.dot_general(a, b, (((1,), (1,)), ((), ())), preferred_element_type=F32)


def sigmoid(x):
    return 1.0 / (1.0 + jnp.exp(-x))


def split_rows(row):
    hi = row.astype(BF16)
    rest = row - hi.astype(F32)
    mid = rest.astype(BF16)
    low = (rest - mid.astype(F32)).astype(BF16)
    rows = lax.broadcasted_iota(jnp.int32, (16, DK), 0)
    return jnp.where(
        rows == 0,
        hi.astype(F32),
        jnp.where(rows == 1, mid.astype(F32), jnp.where(rows == 2, low.astype(F32), 0.0)),
    ).astype(BF16)


def joined_rows(block):
    return jnp.sum(block.astype(F32), axis=0, keepdims=True)


def kernel(
    nz,
    stream, wp, wq, wf, wv, wg, pmix, pscale, lbound, edecay, rgain, wop, wor, ngain, nbias,
    out,
    x_v, wf_v, wv_v, wp_v, wq_v, wg_v, wo_v,
    pmix_v, pscale_v, lb_v, ed_v, rgain_v, ngain_v, nbias_v,
    v_v, explog_v, down_v, pooled_v, halo_v, sq_v, gate_v, a_v,
    st_v, cur_v, off_v, offcur_v, band_v, tri_v,
    s1_send, s1_recv, s2_send, s2_recv, s3_send, s3_recv, pre_v, bsum_v,
    resid_v, stat_v, ostat_v, o_v,
    load_sem, param_sem,
    xs_sem, xr_sem, ws_sem, wr_sem, ps_sem, pr_sem, rs_sem, rr_sem, ss_sem, sr_sem,
    hs_sem, hr_sem, m1s_sem, m1r_sem, m2s_sem, m2r_sem, m3s_sem, m3r_sem, o_sem,
):
    z = lax.axis_index("sp_0")
    x = lax.axis_index("sp_1")
    tp = lax.axis_index("tp")
    sp = z * NX + x
    other = 1 - tp
    n_sp = nz * NX
    after = lax.rem(sp + 1, n_sp)
    prior = lax.rem(sp + n_sp - 1, n_sp)
    partner = {"tp": other}
    x_peers = [{"sp_1": lax.rem(x + d, NX)} for d in range(1, NX)]
    z_peers = [{"sp_0": lax.rem(z + d, nz)} for d in range(1, nz)]
    next_dev = {"sp_0": after // NX, "sp_1": lax.rem(after, NX)}
    prev_dev = {"sp_0": prior // NX, "sp_1": lax.rem(prior, NX)}

    own_rows = pl.ds(pl.multiple_of(tp * H, H), H)
    oth_rows = pl.ds(pl.multiple_of(other * H, H), H)

    def load_tile(c):
        rows = pl.ds(c * R, R)
        return pltpu.make_async_copy(stream.at[rows, :], x_v.at[rows, pl.ds(0, H)], load_sem.at[c])

    loads = [load_tile(c) for c in range(NT)]
    weight_loads = []
    for k, (src, dst) in enumerate(((wf, wf_v), (wv, wv_v), (wp, wp_v), (wq, wq_v), (wg, wg_v))):
        weight_loads.append(
            (
                pltpu.make_async_copy(src.at[own_rows, :], dst.at[pl.ds(0, H), :], load_sem.at[NT + 2 * k]),
                pltpu.make_async_copy(src.at[oth_rows, :], dst.at[pl.ds(H, H), :], load_sem.at[NT + 2 * k + 1]),
            )
        )
    params = [
        pltpu.make_async_copy(src, dst, param_sem.at[k])
        for k, (src, dst) in enumerate(
            (
                (lbound, lb_v), (edecay, ed_v), (pmix, pmix_v), (pscale, pscale_v),
                (rgain, rgain_v), (ngain, ngain_v), (nbias, nbias_v),
            )
        )
    ]
    own_cols = pl.ds(pl.multiple_of(tp * H, H), H)
    oth_cols = pl.ds(pl.multiple_of(other * H, H), H)
    out_loads = [
        pltpu.make_async_copy(src.at[:, own_cols], wo_v.at[pl.ds(k * C, C), :], load_sem.at[NT + 10 + k])
        for k, src in enumerate((wop, wor))
    ]
    loads[0].start()
    weight_loads[0][0].start()
    weight_loads[0][1].start()
    params[0].start()
    params[1].start()
    for c in range(1, NT):
        loads[c].start()
    for pair in weight_loads[1:]:
        pair[0].start()
        pair[1].start()
    for k in range(2, 7):
        params[k].start()
    for c in out_loads:
        c.start()

    barrier = pltpu.get_barrier_semaphore()
    greeted = [partner] + x_peers + z_peers + [next_dev, prev_dev]
    for dev in greeted:
        pl.semaphore_signal(barrier, inc=1, device_id=dev, device_id_type=MESH)
    pl.semaphore_wait(barrier, len(greeted))

    def send(src, dst, s_sem, r_sem, dev):
        return pltpu.make_async_remote_copy(
            src_ref=src, dst_ref=dst, send_sem=s_sem, recv_sem=r_sem, device_id=dev, device_id_type=MESH
        )

    x_sends = [
        send(
            stream.at[pl.ds(c * R, R), :], x_v.at[pl.ds(c * R, R), pl.ds(H, H)],
            xs_sem.at[c], xr_sem.at[c], partner,
        )
        for c in range(NT)
    ]
    for c in x_sends:
        c.start()
    w_sends = [
        send(src.at[:, oth_cols], wo_v.at[pl.ds((2 + k) * C, C), :], ws_sem.at[k], wr_sem.at[k], partner)
        for k, src in enumerate((wop, wor))
    ]
    for c in w_sends:
        c.start()

    row = lax.broadcasted_iota(jnp.int32, (B, B), 0)
    col = lax.broadcasted_iota(jnp.int32, (B, B), 1)
    lower = row >= col
    tri_v[...] = jnp.where(lower, 1.0, 0.0).astype(BF16)
    brow = lax.broadcasted_iota(jnp.int32, (B, 2 * B), 0)
    lag = brow + B - lax.broadcasted_iota(jnp.int32, (B, 2 * B), 1)
    for g in range(2):
        width = jnp.left_shift(2, 2 * tp + g)
        band_v[g] = jnp.where((lag >= 0) & (lag < width), 1.0, 0.0).astype(BF16)
    cur_v[...] = jnp.zeros_like(cur_v)
    offcur_v[...] = jnp.zeros_like(offcur_v)

    params[0].wait()
    params[1].wait()
    weight_loads[0][0].wait()
    weight_loads[0][1].wait()
    weight_loads[1][0].wait()
    weight_loads[1][1].wait()
    for c in range(NT):
        loads[c].wait()
    for c in range(NT):
        x_sends[c].wait_recv()

    @pl.loop(0, NT)
    def _(c):
        r0 = pl.multiple_of(c * R, R)
        xt = x_v[pl.ds(r0, R), :]
        fi = dot(xt, wf_v[...]).astype(BF16).astype(F32)
        vi = dot(xt, wv_v[...]).astype(BF16)
        v_v[pl.ds(r0, R), :] = vi
        gap = 1.0 - lb_v[...]
        w_in = gap * sigmoid(-fi)
        keep = jnp.log(1.0 - w_in)
        for s in range(R // B):
            b = c * (R // B) + s
            rb = pl.multiple_of(r0 + s * B, B)
            rows = slice(s * B, (s + 1) * B)
            ed = ed_v[pl.ds(rb, B), :]
            tri = tri_v[...]
            off = offcur_v[...]
            ends = []
            for h in range(NH):
                hs = slice(h * DK, (h + 1) * DK)
                lk = keep[rows, hs] + ed[:, h : h + 1]
                hi = lk.astype(BF16)
                lo = (lk - hi.astype(F32)).astype(BF16)
                total = dot(tri, hi) + dot(tri, lo)
                end = total[B - 1 : B, :]
                ends.append(end)
                wi = w_in[rows, hs]
                explog_v[pl.ds(rb, B), hs] = jnp.exp(total)
                down_v[pl.ds(rb, B), hs] = (wi * jnp.exp(-total)).astype(BF16)
                inw = (wi * jnp.exp(end - total)).astype(BF16)
                own = dot_tn(vi[rows, hs], inw)
                st = cur_v[h]
                st_v[b, h] = st
                cur_v[h] = jnp.exp(end) * st + own
            off_v[b] = off
            offcur_v[...] = off + jnp.concatenate(ends, axis=1)

    for h in range(NH):
        s1_send[h, pl.ds(0, DK), :] = cur_v[h].astype(BF16)
        s1_send[h, pl.ds(DK, 16), :] = split_rows(offcur_v[0:1, h * DK : (h + 1) * DK])

    def msg1(d):
        to = lax.rem(x + d, NX)
        return send(s1_send.at[to], s1_recv.at[x], m1s_sem.at[d - 1], m1r_sem.at[x], {"sp_1": to})

    def arrival1(d):
        frm = lax.rem(x + d, NX)
        return send(s1_send.at[frm], s1_recv.at[frm], m1s_sem.at[d - 1], m1r_sem.at[frm], {"sp_1": frm})

    for d in range(1, NX):
        msg1(d).start()

    weight_loads[2][0].wait()
    weight_loads[2][1].wait()
    pooled_v[pl.ds(0, B), :] = jnp.zeros((B, C), BF16)

    @pl.loop(0, NT)
    def _(c):
        r0 = pl.multiple_of(c * R, R)
        pooled_v[pl.ds(pl.multiple_of(r0 + B, B), R), :] = dot(
            x_v[pl.ds(r0, R), :], wp_v[...]
        ).astype(BF16)

    halo = send(pooled_v.at[pl.ds(T + B - 16, 16), :], halo_v, hs_sem, hr_sem, next_dev)
    halo.start()

    s1_recv[x] = s1_send[x]
    for d in range(1, NX):
        arrival1(d).wait_recv()
    run = jnp.zeros((DK, DK), F32)
    logs = jnp.zeros((1, DK), F32)
    for k in range(NX):
        pre_v[k] = run
        bsum_v[k] = jnp.broadcast_to(logs, (8, DK))
        a_k = joined_rows(s1_recv[k, pl.ds(DK, 16), :])
        run = jnp.exp(a_k) * run + s1_recv[k, pl.ds(0, DK), :].astype(F32)
        logs = logs + a_k
    s2_send[pl.ds(0, DK), :] = run.astype(BF16)
    s2_send[pl.ds(DK, 16), :] = split_rows(logs)

    def msg2(d):
        to = lax.rem(z + d, nz)
        return send(s2_send, s2_recv.at[z], m2s_sem.at[d - 1], m2r_sem.at[z], {"sp_0": to})

    def arrival2(d):
        frm = lax.rem(z + d, nz)
        return send(s2_send, s2_recv.at[frm], m2s_sem.at[d - 1], m2r_sem.at[frm], {"sp_0": frm})

    for d in range(1, nz):
        msg2(d).start()

    weight_loads[3][0].wait()
    weight_loads[3][1].wait()

    @pl.loop(0, NT)
    def _(c):
        r0 = pl.multiple_of(c * R, R)
        q = dot(x_v[pl.ds(r0, R), :], wq_v[...]).astype(BF16).astype(F32)
        q = q * sigmoid(q)
        up = (q * explog_v[pl.ds(r0, R), :]).astype(BF16)
        for s in range(R // B):
            rb = pl.multiple_of(r0 + s * B, B)
            for h in range(NH):
                hs = slice(h * DK, (h + 1) * DK)
                u = up[s * B : (s + 1) * B, hs]
                sc = dot_nt(u, down_v[pl.ds(rb, B), hs])
                sc = jnp.where(lower, sc, 0.0).astype(BF16)
                sq_v[pl.ds(rb, B), 2 * h * DK : (2 * h + 1) * DK] = sc
                sq_v[pl.ds(rb, B), (2 * h + 1) * DK : (2 * h + 2) * DK] = u

    s2_recv[z] = s2_send[...]
    for d in range(1, nz):
        arrival2(d).wait_recv()
    run = jnp.zeros((DK, DK), F32)
    for k in range(nz - 1):
        b_k = joined_rows(s2_recv[k, pl.ds(DK, 16), :])
        new = jnp.exp(b_k) * run + s2_recv[k, pl.ds(0, DK), :].astype(F32)
        run = jnp.where(k < z, new, run)
    for k in range(NX):
        s3_send[k] = (jnp.exp(bsum_v[k][0:1, :]) * run + pre_v[k]).astype(BF16)

    def msg3(d):
        to = lax.rem(x + d, NX)
        return send(s3_send.at[to], s3_recv.at[x], m3s_sem.at[d - 1], m3r_sem.at[x], {"sp_1": to})

    def arrival3(d):
        frm = lax.rem(x + d, NX)
        return send(s3_send.at[frm], s3_recv.at[frm], m3s_sem.at[d - 1], m3r_sem.at[frm], {"sp_1": frm})

    for d in range(1, NX):
        msg3(d).start()

    weight_loads[4][0].wait()
    weight_loads[4][1].wait()
    for k in range(2, 7):
        params[k].wait()

    @pl.loop(0, NT)
    def _(c):
        r0 = pl.multiple_of(c * R, R)
        g = dot(x_v[pl.ds(r0, R), :], wg_v[...]).astype(BF16).astype(F32)
        gain = jnp.concatenate([rgain_v[...]] * NH, axis=1)
        gate_v[pl.ds(r0, R), :] = g * sigmoid(g) * gain

    halo.wait_recv()
    pooled_v[pl.ds(B - 16, 16), :] = jnp.where(sp > 0, halo_v[...], jnp.zeros_like(halo_v))

    def pool_send(c):
        rows = pl.ds(pl.multiple_of(c * R, R), R)
        return send(a_v.at[rows, pl.ds(0, C)], a_v.at[rows, pl.ds(2 * C, C)], ps_sem.at[c], pr_sem.at[c], partner)

    @pl.loop(0, NT)
    def _(c):
        r0 = pl.multiple_of(c * R, R)
        for s in range(R // B):
            rb = pl.multiple_of(r0 + s * B, B)
            position = sp * T + rb + lax.broadcasted_iota(jnp.int32, (B, 1), 0) + 1
            for g in range(2):
                cols = slice(g * 256, (g + 1) * 256)
                total = dot(band_v[g], pooled_v[pl.ds(rb, 2 * B), cols])
                here = pooled_v[pl.ds(pl.multiple_of(rb + B, B), B), cols].astype(F32)
                width = jnp.left_shift(2, 2 * tp + g)
                count = jnp.minimum(position, width).astype(F32)
                diff = (total / count - here).astype(BF16)
                mixed = dot(diff, pmix_v[g]) * pscale_v[:, cols]
                a_v[pl.ds(rb, B), cols] = mixed.astype(BF16)

    for c in range(NT):
        pool_send(c).start()

    s3_recv[x] = s3_send[x]
    for d in range(1, NX):
        arrival3(d).wait_recv()

    for c in out_loads:
        c.wait()
    for c in w_sends:
        c.wait_recv()
    for c in range(NT):
        pool_send(c).wait_recv()

    def rec_send(c):
        rows = pl.ds(pl.multiple_of(c * R, R), R)
        return send(a_v.at[rows, pl.ds(C, C)], a_v.at[rows, pl.ds(3 * C, C)], rs_sem.at[c], rr_sem.at[c], partner)

    def stat_send(c):
        rows = pl.ds(pl.multiple_of(c * R, R), R)
        return send(stat_v.at[rows, :], ostat_v.at[rows, :], ss_sem.at[c], sr_sem.at[c], partner)

    @pl.loop(0, NT)
    def _(c):
        r0 = pl.multiple_of(c * R, R)
        for s in range(R // B):
            b = c * (R // B) + s
            rb = pl.multiple_of(r0 + s * B, B)
            far = jnp.exp(off_v[b])
            for h in range(NH):
                hs = slice(h * DK, (h + 1) * DK)
                state = st_v[b, h] + far[:, hs] * s3_recv[h].astype(F32)
                raw = dot(sq_v[pl.ds(rb, B), 2 * h * DK : (2 * h + 1) * DK], v_v[pl.ds(rb, B), hs])
                raw = raw + dot_nt(
                    sq_v[pl.ds(rb, B), (2 * h + 1) * DK : (2 * h + 2) * DK], state.astype(BF16)
                )
                power = jnp.mean(raw * raw, axis=1, keepdims=True)
                normed = raw * lax.rsqrt(power + EPS_RMS) * gate_v[pl.ds(rb, B), hs]
                a_v[pl.ds(rb, B), C + h * DK : C + (h + 1) * DK] = normed.astype(BF16)
        rec_send(c).start()

    @pl.loop(0, NT)
    def _(c):
        r0 = pl.multiple_of(c * R, R)
        rec_send(c).wait_recv()
        mix = dot(a_v[pl.ds(r0, R), :], wo_v[...])
        resid = ALPHA * x_v[pl.ds(r0, R), 0:H].astype(F32) + mix
        resid_v[pl.ds(r0, R), :] = resid
        mean = jnp.sum(resid, axis=1, keepdims=True) * (1.0 / H)
        dev = resid - mean
        m2 = jnp.sum(dev * dev, axis=1, keepdims=True)
        lane = lax.broadcasted_iota(jnp.int32, (R, DK), 1)
        stat_v[pl.ds(r0, R), :] = jnp.where(lane == 0, mean, m2)
        stat_send(c).start()

    def out_copy(c):
        rows = pl.ds(pl.multiple_of(c * R, R), R)
        return pltpu.make_async_copy(o_v.at[rows, :], out.at[rows, :], o_sem.at[c])

    @pl.loop(0, NT)
    def _(c):
        r0 = pl.multiple_of(c * R, R)
        stat_send(c).wait_recv()
        mine = stat_v[pl.ds(r0, R), :]
        theirs = ostat_v[pl.ds(r0, R), :]
        gap = mine[:, 0:1] - theirs[:, 0:1]
        mean = 0.5 * (mine[:, 0:1] + theirs[:, 0:1])
        var = (mine[:, 1:2] + theirs[:, 1:2] + gap * gap * (0.5 * H)) * (1.0 / (2 * H))
        scale = lax.rsqrt(var + EPS_NORM)
        o_v[pl.ds(r0, R), :] = (
            (resid_v[pl.ds(r0, R), :] - mean) * scale * ngain_v[...] + nbias_v[...]
        ).astype(BF16)
        out_copy(c).start()

    for c in range(NT):
        out_copy(c).wait()
        x_sends[c].wait_send()
        pool_send(c).wait_send()
        rec_send(c).wait_send()
        stat_send(c).wait_send()
    for c in w_sends:
        c.wait_send()
    halo.wait_send()
    for d in range(1, NX):
        msg1(d).wait_send()
        msg3(d).wait_send()
    for d in range(1, nz):
        msg2(d).wait_send()


def layer(nz, *args):
    (stream, wp, wq, wf, wv, wg, pmix, pscale, lb, ed, rgain, wop, wor, ngain, nbias) = args
    anyspace = pl.BlockSpec(memory_space=pl.ANY)
    sem = pltpu.SemaphoreType.DMA
    scratch = [
        pltpu.VMEM((T, 2 * H), BF16),
        *[pltpu.VMEM((2 * H, C), BF16)] * 5,
        pltpu.VMEM((4 * C, H), BF16),
        pltpu.VMEM((2, 256, 256), BF16),
        pltpu.VMEM((1, C), F32),
        pltpu.VMEM((1, C), F32),
        pltpu.VMEM((T, NH), F32),
        pltpu.VMEM((1, DK), F32),
        pltpu.VMEM((1, H), F32),
        pltpu.VMEM((1, H), F32),
        pltpu.VMEM((T, C), BF16),
        pltpu.VMEM((T, C), F32),
        pltpu.VMEM((T, C), BF16),
        pltpu.VMEM((T + B, C), BF16),
        pltpu.VMEM((16, C), BF16),
        pltpu.VMEM((T, 2 * C), BF16),
        pltpu.VMEM((T, C), F32),
        pltpu.VMEM((T, 4 * C), BF16),
        pltpu.VMEM((NB, NH, DK, DK), F32),
        pltpu.VMEM((NH, DK, DK), F32),
        pltpu.VMEM((NB, 1, C), F32),
        pltpu.VMEM((1, C), F32),
        pltpu.VMEM((2, B, 2 * B), BF16),
        pltpu.VMEM((B, B), BF16),
        pltpu.VMEM((NH, MSG, DK), BF16),
        pltpu.VMEM((NX, MSG, DK), BF16),
        pltpu.VMEM((MSG, DK), BF16),
        pltpu.VMEM((nz, MSG, DK), BF16),
        pltpu.VMEM((NX, DK, DK), BF16),
        pltpu.VMEM((NX, DK, DK), BF16),
        pltpu.VMEM((NX, DK, DK), F32),
        pltpu.VMEM((NX, 8, DK), F32),
        pltpu.VMEM((T, H), F32),
        pltpu.VMEM((T, DK), F32),
        pltpu.VMEM((T, DK), F32),
        pltpu.VMEM((T, H), BF16),
        sem((NT + 12,)), sem((7,)),
        sem((NT,)), sem((NT,)), sem((2,)), sem((2,)), sem((NT,)), sem((NT,)),
        sem((NT,)), sem((NT,)), sem((NT,)), sem((NT,)),
        sem, sem,
        sem((NX - 1,)), sem((NX,)), sem((nz - 1,)), sem((nz,)), sem((NX - 1,)), sem((NX,)),
        sem((NT,)),
    ]
    result = pl.pallas_call(
        functools.partial(kernel, nz),
        out_shape=jax.ShapeDtypeStruct((T, H), BF16),
        in_specs=[anyspace] * 15,
        out_specs=anyspace,
        scratch_shapes=scratch,
        compiler_params=pltpu.CompilerParams(
            collective_id=0, has_side_effects=True, vmem_limit_bytes=66_000_000
        ),
    )(
        stream[0], wp, wq, wf, wv, wg, pmix,
        pscale.reshape(1, C), lb.reshape(1, C), ed, rgain.reshape(1, DK),
        wop, wor, ngain.reshape(1, H), nbias.reshape(1, H),
    )
    return result[None]


def solution(mesh):
    devices = mesh.devices
    nz = devices.shape[0] // NX
    torus = Mesh(
        devices.reshape(nz, NX, mesh.shape["fs"], mesh.shape["tp"]), ("sp_0", "sp_1", "fs", "tp")
    )
    sp = ("sp_0", "sp_1")
    cols = P(None, "tp")
    return jax.shard_map(
        functools.partial(layer, nz),
        mesh=torus,
        in_specs=(
            P("fs", sp, "tp"), cols, cols, cols, cols, cols,
            P("tp", None, None), P("tp"), P("tp"), P(sp, "tp"), P(),
            P("tp", None), P("tp", None), P("tp"), P("tp"),
        ),
        out_specs=P("fs", sp, "tp"),
        check_vma=False,
    )
```

```python
import functools
import math

import jax
import jax.numpy as jnp
from jax import lax
from jax.experimental import pallas as pl
from jax.experimental.pallas import tpu as pltpu
from jax.sharding import Mesh
from jax.sharding import PartitionSpec as P

BF16 = jnp.bfloat16
F32 = jnp.float32
MESH = pl.DeviceIdType.MESH

ALPHA = 2.0**0.25
EPS_RMS = 1e-06
EPS_NORM = 1e-05
LOG2E = math.log2(math.e)

T = 1024
H = 1024
C = 512
DK = 128
NH = C // DK
B = 128
NB = T // B
R = 256
NT = T // R
NX = 4
MSG = DK + 16


def dot(a, b):
    return jnp.dot(a, b, preferred_element_type=F32)


def dot_tn(a, b):
    return lax.dot_general(a, b, (((0,), (0,)), ((), ())), preferred_element_type=F32)


def dot_nt(a, b):
    return lax.dot_general(a, b, (((1,), (1,)), ((), ())), preferred_element_type=F32)


def silu(x):
    half = 0.5 * x
    return half + half * jnp.tanh(half)


def split_rows(row):
    hi = row.astype(BF16)
    rest = row - hi.astype(F32)
    mid = rest.astype(BF16)
    low = (rest - mid.astype(F32)).astype(BF16)
    rows = lax.broadcasted_iota(jnp.int32, (16, DK), 0)
    return jnp.where(
        rows == 0,
        hi.astype(F32),
        jnp.where(rows == 1, mid.astype(F32), jnp.where(rows == 2, low.astype(F32), 0.0)),
    ).astype(BF16)


def joined_rows(block):
    return jnp.sum(block.astype(F32), axis=0, keepdims=True)


def kernel(
    nz,
    stream, wp, wq, wf, wv, wg, pmix, pscale, lbound, edecay, rgain, wop, wor, ngain, nbias,
    out,
    x_v, wf_v, wv_v, wp_v, wq_v, wg_v, wo_v,
    pmix_v, pscale_v, lb_v, ed_v, edc_v, rgain_v, ngain_v, nbias_v,
    f_v, v_v, explog_v, down_v, pooled_v, halo_v, sq_v, gate_v, a_v,
    st_v, cur_v, off_v, offcur_v, band_v, tri_v,
    s1_send, s1_recv, s2_send, s2_recv, s3_send, s3_recv, pre_v, bsum_v,
    resid_v, stat_v, ostat_v,
    load_sem, param_sem,
    xs_sem, xr_sem, ws_sem, wr_sem, ps_sem, pr_sem, rs_sem, rr_sem, ss_sem, sr_sem,
    hs_sem, hr_sem, m1s_sem, m1r_sem, m2s_sem, m2r_sem, m3s_sem, m3r_sem,
):
    z = lax.axis_index("sp_0")
    x = lax.axis_index("sp_1")
    tp = lax.axis_index("tp")
    sp = z * NX + x
    other = 1 - tp
    n_sp = nz * NX
    after = lax.rem(sp + 1, n_sp)
    prior = lax.rem(sp + n_sp - 1, n_sp)
    partner = {"tp": other}
    x_peers = [{"sp_1": lax.rem(x + d, NX)} for d in range(1, NX)]
    z_peers = [{"sp_0": lax.rem(z + d, nz)} for d in range(1, nz)]
    next_dev = {"sp_0": after // NX, "sp_1": lax.rem(after, NX)}
    prev_dev = {"sp_0": prior // NX, "sp_1": lax.rem(prior, NX)}

    barrier = pltpu.get_barrier_semaphore()
    greeted = [partner] + x_peers + z_peers + [next_dev, prev_dev]
    for dev in greeted:
        pl.semaphore_signal(barrier, inc=1, device_id=dev, device_id_type=MESH)

    own_half = pl.ds(pl.multiple_of(tp * H, H), H)
    oth_half = pl.ds(pl.multiple_of(other * H, H), H)

    def tile(c):
        return pl.ds(c * R, R)

    loads = [
        pltpu.make_async_copy(stream.at[tile(c), :], x_v.at[tile(c), pl.ds(0, H)], load_sem.at[c])
        for c in range(NT)
    ]
    first, second = {}, {}
    for k, (src, dst) in enumerate(((wf, wf_v), (wv, wv_v), (wp, wp_v), (wq, wq_v), (wg, wg_v))):
        first[k] = pltpu.make_async_copy(
            src.at[own_half, :], dst.at[pl.ds(0, H), :], load_sem.at[NT + 2 * k]
        )
        second[k] = pltpu.make_async_copy(
            src.at[oth_half, :], dst.at[pl.ds(H, H), :], load_sem.at[NT + 2 * k + 1]
        )
    params = [
        pltpu.make_async_copy(src, dst, param_sem.at[k])
        for k, (src, dst) in enumerate(
            (
                (lbound, lb_v), (edecay, ed_v), (pmix, pmix_v), (pscale, pscale_v),
                (rgain, rgain_v), (ngain, ngain_v), (nbias, nbias_v),
            )
        )
    ]
    out_loads = [
        pltpu.make_async_copy(
            src.at[:, own_half], wo_v.at[pl.ds(2 * k * C, C), :], load_sem.at[NT + 10 + k]
        )
        for k, src in enumerate((wop, wor))
    ]
    loads[0].start()
    first[0].start()
    for c in range(1, NT):
        loads[c].start()
    first[1].start()
    first[2].start()
    first[3].start()
    for k in range(7):
        params[k].start()
    second[0].start()
    second[1].start()
    second[2].start()
    second[3].start()
    first[4].start()
    second[4].start()
    for c in out_loads:
        c.start()

    row = lax.broadcasted_iota(jnp.int32, (B, B), 0)
    col = lax.broadcasted_iota(jnp.int32, (B, B), 1)
    lower = row >= col
    ones = jnp.where(lower, 1.0, 0.0).astype(BF16)
    tri_v[:, 0:B] = ones
    tri_v[:, B : 2 * B] = ones
    brow = lax.broadcasted_iota(jnp.int32, (B, 2 * B), 0)
    lag = brow + B - lax.broadcasted_iota(jnp.int32, (B, 2 * B), 1)
    for g in range(2):
        width = jnp.left_shift(2, 2 * tp + g)
        band_v[g] = jnp.where((lag >= 0) & (lag < width), 1.0, 0.0).astype(BF16)
    cur_v[...] = jnp.zeros_like(cur_v)
    offcur_v[...] = jnp.zeros_like(offcur_v)
    pooled_v[pl.ds(0, B), :] = jnp.zeros((B, C), BF16)

    first[0].wait()
    for c in range(NT):
        loads[c].wait()
        f_v[tile(c), :] = dot(x_v[tile(c), 0:H], wf_v[0:H, :])

    first[1].wait()
    for c in range(NT):
        resid_v[tile(c), 0:C] = dot(x_v[tile(c), 0:H], wv_v[0:H, :])
    pl.semaphore_wait(barrier, len(greeted))

    def send(src, dst, s_sem, r_sem, dev):
        return pltpu.make_async_remote_copy(
            src_ref=src, dst_ref=dst, send_sem=s_sem, recv_sem=r_sem, device_id=dev, device_id_type=MESH
        )

    x_sends = [
        send(
            x_v.at[tile(c), pl.ds(0, H)], x_v.at[tile(c), pl.ds(H, H)],
            xs_sem.at[c], xr_sem.at[c], partner,
        )
        for c in range(NT)
    ]
    for c in x_sends:
        c.start()
    w_sends = [
        send(
            src.at[:, oth_half], wo_v.at[pl.ds((2 * k + 1) * C, C), :], ws_sem.at[k], wr_sem.at[k], partner
        )
        for k, src in enumerate((wop, wor))
    ]

    first[2].wait()
    for c in range(NT):
        resid_v[tile(c), C : 2 * C] = dot(x_v[tile(c), 0:H], wp_v[0:H, :])
    first[3].wait()
    for c in range(NT):
        gate_v[tile(c), :] = dot(x_v[tile(c), 0:H], wq_v[0:H, :])
    params[0].wait()
    params[1].wait()
    for b in range(NB):
        edc_v[pl.ds(b * B, B), :] = jnp.transpose(ed_v[:, b * B : (b + 1) * B] * LOG2E)

    def forget_dots(c):
        f_v[tile(c), :] = f_v[tile(c), :] + dot(x_v[tile(c), H : 2 * H], wf_v[H : 2 * H, :])
        v_v[tile(c), :] = (
            resid_v[tile(c), 0:C] + dot(x_v[tile(c), H : 2 * H], wv_v[H : 2 * H, :])
        ).astype(BF16)

    def forget_block(b):
        rows = pl.ds(b * B, B)
        ed = edc_v[rows, :]
        off = offcur_v[...]
        off_v[b] = off
        for p in range(NH // 2):
            cols = slice(2 * p * DK, 2 * (p + 1) * DK)
            half_gap = 0.5 - 0.5 * lb_v[:, cols]
            f = f_v[rows, cols].astype(BF16).astype(F32)
            w_in = half_gap - half_gap * jnp.tanh(0.5 * f)
            keep = jnp.log(1.0 - w_in) * LOG2E
            keep = jnp.concatenate(
                [keep[:, k * DK : (k + 1) * DK] + ed[:, 2 * p + k : 2 * p + k + 1] for k in range(2)], axis=1
            )
            hi = keep.astype(BF16)
            lo = (keep - hi.astype(F32)).astype(BF16)
            total = dot(tri_v[...], jnp.concatenate([hi, lo], axis=0))
            end = total[B - 1 : B, :]
            explog_v[rows, cols] = jnp.exp2(total)
            down_v[rows, cols] = (w_in * jnp.exp2(-total)).astype(BF16)
            inw = (w_in * jnp.exp2(end - total)).astype(BF16)
            kept = jnp.exp2(end)
            offcur_v[:, cols] = off[:, cols] + end
            for k in range(2):
                h = 2 * p + k
                hs = slice(k * DK, (k + 1) * DK)
                st = cur_v[h]
                st_v[b, h] = st
                cur_v[h] = kept[:, hs] * st + dot_tn(v_v[rows, h * DK : (h + 1) * DK], inw[:, hs])

    second[0].wait()
    second[1].wait()
    x_sends[0].wait_recv()
    forget_dots(0)
    for c in range(NT):
        if c + 1 < NT:
            x_sends[c + 1].wait_recv()
            forget_dots(c + 1)
        for s in range(R // B):
            forget_block(c * (R // B) + s)

    for h in range(NH):
        s1_send[h, pl.ds(0, DK), :] = cur_v[h].astype(BF16)
        s1_send[h, pl.ds(DK, 16), :] = split_rows(offcur_v[0:1, h * DK : (h + 1) * DK])

    def msg1(d):
        to = lax.rem(x + d, NX)
        return send(s1_send.at[to], s1_recv.at[x], m1s_sem.at[d - 1], m1r_sem.at[x], {"sp_1": to})

    def arrival1(d):
        frm = lax.rem(x + d, NX)
        return send(s1_send.at[frm], s1_recv.at[frm], m1s_sem.at[d - 1], m1r_sem.at[frm], {"sp_1": frm})

    for d in range(1, NX):
        msg1(d).start()
    for c in w_sends:
        c.start()

    second[2].wait()
    for c in range(NT):
        pooled_v[pl.ds(c * R + B, R), :] = (
            resid_v[tile(c), C : 2 * C] + dot(x_v[tile(c), H : 2 * H], wp_v[H : 2 * H, :])
        ).astype(BF16)

    halo = send(pooled_v.at[pl.ds(T + B - 16, 16), :], halo_v, hs_sem, hr_sem, next_dev)
    halo.start()

    second[3].wait()

    def query_dots(c):
        q = gate_v[tile(c), :] + dot(x_v[tile(c), H : 2 * H], wq_v[H : 2 * H, :])
        q = q.astype(BF16).astype(F32)
        up = (silu(q) * explog_v[tile(c), :]).astype(BF16)
        for s in range(R // B):
            rows = pl.ds(c * R + s * B, B)
            for h in range(NH):
                hs = slice(h * DK, (h + 1) * DK)
                u = up[s * B : (s + 1) * B, hs]
                sc = dot_nt(u, down_v[rows, hs])
                sq_v[rows, 2 * h * DK : (2 * h + 1) * DK] = jnp.where(lower, sc, 0.0).astype(BF16)
                sq_v[rows, (2 * h + 1) * DK : (2 * h + 2) * DK] = u

    for c in range(NT):
        query_dots(c)

    s1_recv[x] = s1_send[x]
    for d in range(1, NX):
        arrival1(d).wait_recv()
    run = jnp.zeros((DK, DK), F32)
    logs = jnp.zeros((1, DK), F32)
    for k in range(NX):
        pre_v[k] = run
        bsum_v[k] = jnp.broadcast_to(logs, (8, DK))
        a_k = joined_rows(s1_recv[k, pl.ds(DK, 16), :])
        run = jnp.exp2(a_k) * run + s1_recv[k, pl.ds(0, DK), :].astype(F32)
        logs = logs + a_k
    s2_send[pl.ds(0, DK), :] = run.astype(BF16)
    s2_send[pl.ds(DK, 16), :] = split_rows(logs)

    def msg2(d):
        to = lax.rem(z + d, nz)
        return send(s2_send, s2_recv.at[z], m2s_sem.at[d - 1], m2r_sem.at[z], {"sp_0": to})

    def arrival2(d):
        frm = lax.rem(z + d, nz)
        return send(s2_send, s2_recv.at[frm], m2s_sem.at[d - 1], m2r_sem.at[frm], {"sp_0": frm})

    for d in range(1, nz):
        msg2(d).start()

    first[4].wait()
    second[4].wait()
    for k in range(2, 7):
        params[k].wait()

    def gate_dots(c):
        g = dot(x_v[tile(c), :], wg_v[...]).astype(BF16).astype(F32)
        gain = jnp.concatenate([rgain_v[...]] * NH, axis=1)
        gate_v[tile(c), :] = silu(g) * gain

    for c in range(NT):
        gate_dots(c)

    s2_recv[z] = s2_send[...]
    for d in range(1, nz):
        arrival2(d).wait_recv()
    run = jnp.zeros((DK, DK), F32)
    for k in range(nz - 1):
        b_k = joined_rows(s2_recv[k, pl.ds(DK, 16), :])
        new = jnp.exp2(b_k) * run + s2_recv[k, pl.ds(0, DK), :].astype(F32)
        run = jnp.where(k < z, new, run)
    for k in range(NX):
        s3_send[k] = (jnp.exp2(bsum_v[k][0:1, :]) * run + pre_v[k]).astype(BF16)

    def msg3(d):
        to = lax.rem(x + d, NX)
        return send(s3_send.at[to], s3_recv.at[x], m3s_sem.at[d - 1], m3r_sem.at[x], {"sp_1": to})

    def arrival3(d):
        frm = lax.rem(x + d, NX)
        return send(s3_send.at[frm], s3_recv.at[frm], m3s_sem.at[d - 1], m3r_sem.at[frm], {"sp_1": frm})

    for d in range(1, NX):
        msg3(d).start()

    halo.wait_recv()
    pooled_v[pl.ds(B - 16, 16), :] = jnp.where(sp > 0, halo_v[...], jnp.zeros_like(halo_v))

    pool_sends = [
        send(a_v.at[tile(c), pl.ds(0, C)], a_v.at[tile(c), pl.ds(C, C)], ps_sem.at[c], pr_sem.at[c], partner)
        for c in range(NT)
    ]

    def pooling(b):
        position = sp * T + b * B + lax.broadcasted_iota(jnp.int32, (B, 1), 0) + 1
        for g in range(2):
            cols = slice(g * 256, (g + 1) * 256)
            total = dot(band_v[g], pooled_v[pl.ds(b * B, 2 * B), cols])
            here = pooled_v[pl.ds((b + 1) * B, B), cols].astype(F32)
            width = jnp.left_shift(2, 2 * tp + g)
            if b == 0:
                diff = total / jnp.minimum(position, width).astype(F32) - here
            else:
                diff = total * (1.0 / width.astype(F32)) - here
            mixed = dot(diff.astype(BF16), pmix_v[g]) * pscale_v[:, cols]
            a_v[pl.ds(b * B, B), cols] = mixed.astype(BF16)

    for c in range(NT):
        for s in range(R // B):
            pooling(c * (R // B) + s)
        pool_sends[c].start()

    for c in out_loads:
        c.wait()
    for c in w_sends:
        c.wait_recv()
    for c in range(NT):
        pool_sends[c].wait_recv()
        resid_v[tile(c), :] = ALPHA * x_v[tile(c), 0:H].astype(F32) + dot(
            a_v[tile(c), 0 : 2 * C], wo_v[0 : 2 * C, :]
        )

    s3_recv[x] = s3_send[x]
    for d in range(1, NX):
        arrival3(d).wait_recv()

    rec_sends = [
        send(
            a_v.at[tile(c), pl.ds(2 * C, C)], a_v.at[tile(c), pl.ds(3 * C, C)],
            rs_sem.at[c], rr_sem.at[c], partner,
        )
        for c in range(NT)
    ]
    stat_sends = [
        send(stat_v.at[tile(c), :], ostat_v.at[tile(c), :], ss_sem.at[c], sr_sem.at[c], partner)
        for c in range(NT)
    ]

    def recur(b):
        rows = pl.ds(b * B, B)
        far = jnp.exp2(off_v[b])
        for h in range(NH):
            hs = slice(h * DK, (h + 1) * DK)
            state = st_v[b, h] + far[:, hs] * s3_recv[h].astype(F32)
            raw = dot(sq_v[rows, 2 * h * DK : (2 * h + 1) * DK], v_v[rows, hs])
            raw = raw + dot_nt(sq_v[rows, (2 * h + 1) * DK : (2 * h + 2) * DK], state.astype(BF16))
            power = jnp.mean(raw * raw, axis=1, keepdims=True)
            normed = raw * lax.rsqrt(power + EPS_RMS) * gate_v[rows, hs]
            a_v[rows, 2 * C + h * DK : 2 * C + (h + 1) * DK] = normed.astype(BF16)

    def project(c):
        resid = resid_v[tile(c), :] + dot(a_v[tile(c), 2 * C : 4 * C], wo_v[2 * C : 4 * C, :])
        resid_v[tile(c), :] = resid
        mean = jnp.sum(resid, axis=1, keepdims=True) * (1.0 / H)
        dev = resid - mean
        m2 = jnp.sum(dev * dev, axis=1, keepdims=True)
        lane = lax.broadcasted_iota(jnp.int32, (R, DK), 1)
        stat_v[tile(c), :] = jnp.where(lane == 0, mean, m2)

    def norm(c):
        mine = stat_v[tile(c), :]
        theirs = ostat_v[tile(c), :]
        gap = mine[:, 0:1] - theirs[:, 0:1]
        mean = 0.5 * (mine[:, 0:1] + theirs[:, 0:1])
        var = (mine[:, 1:2] + theirs[:, 1:2] + gap * gap * (0.5 * H)) * (1.0 / (2 * H))
        scale = lax.rsqrt(var + EPS_NORM)
        out[tile(c), :] = (
            (resid_v[tile(c), :] - mean) * scale * ngain_v[...] + nbias_v[...]
        ).astype(BF16)

    for j in range(-2, NT + 2):
        if 0 <= j < NT:
            rec_sends[j].wait_recv()
        if j >= 2:
            stat_sends[j - 2].wait_recv()
        if j + 2 < NT:
            for s in range(R // B):
                recur((j + 2) * (R // B) + s)
        if 0 <= j < NT:
            project(j)
        if j >= 2:
            norm(j - 2)
        if j + 2 < NT:
            rec_sends[j + 2].start()
        if 0 <= j < NT:
            stat_sends[j].start()

    for c in range(NT):
        x_sends[c].wait_send()
        pool_sends[c].wait_send()
        rec_sends[c].wait_send()
        stat_sends[c].wait_send()
    for c in w_sends:
        c.wait_send()
    halo.wait_send()
    for d in range(1, NX):
        msg1(d).wait_send()
        msg3(d).wait_send()
    for d in range(1, nz):
        msg2(d).wait_send()


def layer(nz, *args):
    (stream, wp, wq, wf, wv, wg, pmix, pscale, lb, ed, rgain, wop, wor, ngain, nbias) = args
    sem = pltpu.SemaphoreType.DMA
    scratch = [
        pltpu.VMEM((T, 2 * H), BF16),
        *[pltpu.VMEM((2 * H, C), BF16)] * 5,
        pltpu.VMEM((4 * C, H), BF16),
        pltpu.VMEM((2, 256, 256), BF16),
        pltpu.VMEM((1, C), F32),
        pltpu.VMEM((1, C), F32),
        pltpu.VMEM((NH, T), F32),
        pltpu.VMEM((T, NH), F32),
        pltpu.VMEM((1, DK), F32),
        pltpu.VMEM((1, H), F32),
        pltpu.VMEM((1, H), F32),
        pltpu.VMEM((T, C), F32),
        pltpu.VMEM((T, C), BF16),
        pltpu.VMEM((T, C), F32),
        pltpu.VMEM((T, C), BF16),
        pltpu.VMEM((T + B, C), BF16),
        pltpu.VMEM((16, C), BF16),
        pltpu.VMEM((T, 2 * C), BF16),
        pltpu.VMEM((T, C), F32),
        pltpu.VMEM((T, 4 * C), BF16),
        pltpu.VMEM((NB, NH, DK, DK), F32),
        pltpu.VMEM((NH, DK, DK), F32),
        pltpu.VMEM((NB, 1, C), F32),
        pltpu.VMEM((1, C), F32),
        pltpu.VMEM((2, B, 2 * B), BF16),
        pltpu.VMEM((B, 2 * B), BF16),
        pltpu.VMEM((NH, MSG, DK), BF16),
        pltpu.VMEM((NX, MSG, DK), BF16),
        pltpu.VMEM((MSG, DK), BF16),
        pltpu.VMEM((nz, MSG, DK), BF16),
        pltpu.VMEM((NX, DK, DK), BF16),
        pltpu.VMEM((NX, DK, DK), BF16),
        pltpu.VMEM((NX, DK, DK), F32),
        pltpu.VMEM((NX, 8, DK), F32),
        pltpu.VMEM((T, H), F32),
        pltpu.VMEM((T, DK), F32),
        pltpu.VMEM((T, DK), F32),
        sem((NT + 12,)), sem((7,)),
        sem((NT,)), sem((NT,)), sem((2,)), sem((2,)), sem((NT,)), sem((NT,)),
        sem((NT,)), sem((NT,)), sem((NT,)), sem((NT,)),
        sem, sem,
        sem((NX - 1,)), sem((NX,)), sem((nz - 1,)), sem((nz,)), sem((NX - 1,)), sem((NX,)),
    ]
    operands = (
        stream[0], wp, wq, wf, wv, wg, pmix,
        pscale.reshape(1, C), lb.reshape(1, C), ed.T, rgain.reshape(1, DK),
        wop, wor, ngain.reshape(1, H), nbias.reshape(1, H),
    )
    result = pl.pallas_call(
        functools.partial(kernel, nz),
        out_shape=pltpu.VMEM((T, H), BF16),
        in_specs=[pl.BlockSpec(memory_space=pltpu.HBM)] * 15,
        out_specs=pl.BlockSpec(memory_space=pltpu.VMEM),
        scratch_shapes=scratch,
        compiler_params=pltpu.CompilerParams(
            collective_id=0, has_side_effects=True, vmem_limit_bytes=58_000_000
        ),
    )(*[pltpu.with_memory_space_constraint(a, pltpu.HBM) for a in operands])
    return result[None]


def solution(mesh):
    devices = mesh.devices
    nz = devices.shape[0] // NX
    torus = Mesh(
        devices.reshape(nz, NX, mesh.shape["fs"], mesh.shape["tp"]), ("sp_0", "sp_1", "fs", "tp")
    )
    sp = ("sp_0", "sp_1")
    cols = P(None, "tp")
    return jax.shard_map(
        functools.partial(layer, nz),
        mesh=torus,
        in_specs=(
            P("fs", sp, "tp"), cols, cols, cols, cols, cols,
            P("tp", None, None), P("tp"), P("tp"), P(sp, "tp"), P(),
            P("tp", None), P("tp", None), P("tp"), P("tp"),
        ),
        out_specs=P("fs", sp, "tp"),
        check_vma=False,
    )
```

```python
import functools
import math

import jax
import jax.numpy as jnp
from jax import lax
from jax.experimental import pallas as pl
from jax.experimental.pallas import tpu as pltpu
from jax.sharding import Mesh
from jax.sharding import PartitionSpec as P

BF16 = jnp.bfloat16
F32 = jnp.float32
MESH = pl.DeviceIdType.MESH

ALPHA = 2.0**0.25
EPS_RMS = 1e-06
EPS_NORM = 1e-05
LOG2E = math.log2(math.e)

T = 1024
H = 1024
C = 512
DK = 128
NH = C // DK
B = 128
NB = T // B
R = 256
NT = T // R
NX = 4
MSG = DK + 16


def dot(a, b):
    return jnp.dot(a, b, preferred_element_type=F32)


def dot_tn(a, b):
    return lax.dot_general(a, b, (((0,), (0,)), ((), ())), preferred_element_type=F32)


def dot_nt(a, b):
    return lax.dot_general(a, b, (((1,), (1,)), ((), ())), preferred_element_type=F32)


def silu(x):
    half = 0.5 * x
    return half + half * jnp.tanh(half)


def split_rows(row):
    hi = row.astype(BF16)
    rest = row - hi.astype(F32)
    mid = rest.astype(BF16)
    low = (rest - mid.astype(F32)).astype(BF16)
    rows = lax.broadcasted_iota(jnp.int32, (16, DK), 0)
    return jnp.where(
        rows == 0,
        hi.astype(F32),
        jnp.where(rows == 1, mid.astype(F32), jnp.where(rows == 2, low.astype(F32), 0.0)),
    ).astype(BF16)


def joined_rows(block):
    return jnp.sum(block.astype(F32), axis=0, keepdims=True)


def kernel(
    nz,
    stream, wp, wq, wf, wv, wg, pmix, pscale, lbound, edecay, rgain, wop, wor, ngain, nbias,
    out,
    x_v, wf_v, wv_v, wp_v, wq_v, wg_v, wo_v,
    pmix_v, pscale_v, lb_v, ed_v, edc_v, rgain_v, ngain_v, nbias_v,
    f_v, v_v, explog_v, down_v, pooled_v, halo_v, sq_v, gate_v, a_v,
    st_v, cur_v, off_v, offcur_v, band_v, tri_v,
    s1_send, s1_recv, s2_send, s2_recv, s3_send, s3_recv, pre_v, bsum_v, run_v,
    resid_v, stat_v, ostat_v,
    load_sem, param_sem,
    xs_sem, xr_sem, ws_sem, wr_sem, ps_sem, pr_sem, rs_sem, rr_sem, ss_sem, sr_sem,
    hs_sem, hr_sem, m1s_sem, m1r_sem, m2s_sem, m2r_sem, m3s_sem, m3r_sem,
):
    z = lax.axis_index("sp_0")
    x = lax.axis_index("sp_1")
    tp = lax.axis_index("tp")
    sp = z * NX + x
    other = 1 - tp
    n_sp = nz * NX
    after = lax.rem(sp + 1, n_sp)
    prior = lax.rem(sp + n_sp - 1, n_sp)
    is_first, is_last = sp == 0, sp == n_sp - 1
    partner = {"tp": other}
    x_peers = [{"sp_1": lax.rem(x + d, NX)} for d in range(1, NX)]
    z_peers = [{"sp_0": lax.rem(z + d, nz)} for d in range(1, nz)]
    next_dev = {"sp_0": after // NX, "sp_1": lax.rem(after, NX)}
    prev_dev = {"sp_0": prior // NX, "sp_1": lax.rem(prior, NX)}

    barrier = pltpu.get_barrier_semaphore()
    greeted = [partner] + x_peers + z_peers
    for dev in greeted:
        pl.semaphore_signal(barrier, inc=1, device_id=dev, device_id_type=MESH)

    @pl.when(jnp.logical_not(is_last))
    def _():
        pl.semaphore_signal(barrier, inc=1, device_id=next_dev, device_id_type=MESH)

    @pl.when(jnp.logical_not(is_first))
    def _():
        pl.semaphore_signal(barrier, inc=1, device_id=prev_dev, device_id_type=MESH)


    own_half = pl.ds(pl.multiple_of(tp * H, H), H)
    oth_half = pl.ds(pl.multiple_of(other * H, H), H)

    def tile(c):
        return pl.ds(c * R, R)

    loads = [
        pltpu.make_async_copy(stream.at[tile(c), :], x_v.at[tile(c), pl.ds(0, H)], load_sem.at[c])
        for c in range(NT)
    ]
    first, second = {}, {}
    for k, (src, dst) in enumerate(((wf, wf_v), (wv, wv_v), (wp, wp_v), (wq, wq_v), (wg, wg_v))):
        first[k] = pltpu.make_async_copy(
            src.at[own_half, :], dst.at[pl.ds(0, H), :], load_sem.at[NT + 2 * k]
        )
        second[k] = pltpu.make_async_copy(
            src.at[oth_half, :], dst.at[pl.ds(H, H), :], load_sem.at[NT + 2 * k + 1]
        )
    params = [
        pltpu.make_async_copy(src, dst, param_sem.at[k])
        for k, (src, dst) in enumerate(
            (
                (lbound, lb_v), (edecay, ed_v), (pmix, pmix_v), (pscale, pscale_v),
                (rgain, rgain_v), (ngain, ngain_v), (nbias, nbias_v),
            )
        )
    ]
    out_loads = [
        pltpu.make_async_copy(
            src.at[:, own_half], wo_v.at[pl.ds(2 * k * C, C), :], load_sem.at[NT + 10 + k]
        )
        for k, src in enumerate((wop, wor))
    ]
    loads[0].start()
    first[0].start()
    for c in range(1, NT):
        loads[c].start()
    first[1].start()
    first[2].start()
    first[3].start()
    for k in range(7):
        params[k].start()
    second[0].start()
    second[1].start()
    second[2].start()
    second[3].start()
    first[4].start()
    second[4].start()
    for c in out_loads:
        c.start()

    row = lax.broadcasted_iota(jnp.int32, (B, B), 0)
    col = lax.broadcasted_iota(jnp.int32, (B, B), 1)
    lower = row >= col
    ones = jnp.where(lower, 1.0, 0.0).astype(BF16)
    tri_v[:, 0:B] = ones
    tri_v[:, B : 2 * B] = ones
    brow = lax.broadcasted_iota(jnp.int32, (B, 2 * B), 0)
    lag = brow + B - lax.broadcasted_iota(jnp.int32, (B, 2 * B), 1)
    for g in range(2):
        width = jnp.left_shift(2, 2 * tp + g)
        band_v[g] = jnp.where((lag >= 0) & (lag < width), 1.0, 0.0).astype(BF16)
    cur_v[...] = jnp.zeros_like(cur_v)
    offcur_v[...] = jnp.zeros_like(offcur_v)
    pooled_v[pl.ds(0, B), :] = jnp.zeros((B, C), BF16)

    first[0].wait()
    for c in range(NT):
        loads[c].wait()
        f_v[tile(c), :] = dot(x_v[tile(c), 0:H], wf_v[0:H, :])

    first[1].wait()
    for c in range(NT):
        resid_v[tile(c), 0:C] = dot(x_v[tile(c), 0:H], wv_v[0:H, :])
    pl.semaphore_wait(barrier, len(greeted) + jnp.minimum(sp, 1) + jnp.minimum(n_sp - 1 - sp, 1))

    def send(src, dst, s_sem, r_sem, dev):
        return pltpu.make_async_remote_copy(
            src_ref=src, dst_ref=dst, send_sem=s_sem, recv_sem=r_sem, device_id=dev, device_id_type=MESH
        )

    x_sends = [
        send(
            x_v.at[tile(c), pl.ds(0, H)], x_v.at[tile(c), pl.ds(H, H)],
            xs_sem.at[c], xr_sem.at[c], partner,
        )
        for c in range(NT)
    ]
    for c in x_sends:
        c.start()
    w_sends = [
        send(
            src.at[:, oth_half], wo_v.at[pl.ds((2 * k + 1) * C, C), :], ws_sem.at[k], wr_sem.at[k], partner
        )
        for k, src in enumerate((wop, wor))
    ]

    first[2].wait()
    for c in range(NT):
        resid_v[tile(c), C : 2 * C] = dot(x_v[tile(c), 0:H], wp_v[0:H, :])
    first[3].wait()
    for c in range(NT):
        gate_v[tile(c), :] = dot(x_v[tile(c), 0:H], wq_v[0:H, :])
    params[0].wait()
    params[1].wait()
    for b in range(NB):
        edc_v[pl.ds(b * B, B), :] = jnp.transpose(ed_v[:, b * B : (b + 1) * B] * LOG2E)

    def forget_dots(c):
        f_v[tile(c), :] = f_v[tile(c), :] + dot(x_v[tile(c), H : 2 * H], wf_v[H : 2 * H, :])
        v_v[tile(c), :] = (
            resid_v[tile(c), 0:C] + dot(x_v[tile(c), H : 2 * H], wv_v[H : 2 * H, :])
        ).astype(BF16)

    def forget_block(b):
        rows = pl.ds(b * B, B)
        ed = edc_v[rows, :]
        off = offcur_v[...]
        off_v[b] = off
        for p in range(NH // 2):
            cols = slice(2 * p * DK, 2 * (p + 1) * DK)
            half_gap = 0.5 - 0.5 * lb_v[:, cols]
            f = f_v[rows, cols].astype(BF16).astype(F32)
            w_in = half_gap - half_gap * jnp.tanh(0.5 * f)
            keep = jnp.log(1.0 - w_in) * LOG2E
            keep = jnp.concatenate(
                [keep[:, k * DK : (k + 1) * DK] + ed[:, 2 * p + k : 2 * p + k + 1] for k in range(2)], axis=1
            )
            hi = keep.astype(BF16)
            lo = (keep - hi.astype(F32)).astype(BF16)
            total = dot(tri_v[...], jnp.concatenate([hi, lo], axis=0))
            end = total[B - 1 : B, :]
            explog_v[rows, cols] = jnp.exp2(total)
            down_v[rows, cols] = (w_in * jnp.exp2(-total)).astype(BF16)
            inw = (w_in * jnp.exp2(end - total)).astype(BF16)
            kept = jnp.exp2(end)
            offcur_v[:, cols] = off[:, cols] + end
            for k in range(2):
                h = 2 * p + k
                hs = slice(k * DK, (k + 1) * DK)
                st = cur_v[h]
                st_v[b, h] = st
                cur_v[h] = kept[:, hs] * st + dot_tn(v_v[rows, h * DK : (h + 1) * DK], inw[:, hs])

    second[0].wait()
    second[1].wait()
    x_sends[0].wait_recv()
    forget_dots(0)
    for c in range(NT):
        if c + 1 < NT:
            x_sends[c + 1].wait_recv()
            forget_dots(c + 1)
        for s in range(R // B):
            forget_block(c * (R // B) + s)

    for h in range(NH):
        s1_send[h, pl.ds(0, DK), :] = cur_v[h].astype(BF16)
        s1_send[h, pl.ds(DK, 16), :] = split_rows(offcur_v[0:1, h * DK : (h + 1) * DK])

    def msg1(d):
        to = lax.rem(x + d, NX)
        return send(s1_send.at[to], s1_recv.at[x], m1s_sem.at[d - 1], m1r_sem.at[x], {"sp_1": to})

    def arrival1(d):
        frm = lax.rem(x + d, NX)
        return send(s1_send.at[frm], s1_recv.at[frm], m1s_sem.at[d - 1], m1r_sem.at[frm], {"sp_1": frm})

    for d in range(1, NX):
        msg1(d).start()
    for c in w_sends:
        c.start()

    second[2].wait()
    for c in range(NT):
        pooled_v[pl.ds(c * R + B, R), :] = (
            resid_v[tile(c), C : 2 * C] + dot(x_v[tile(c), H : 2 * H], wp_v[H : 2 * H, :])
        ).astype(BF16)

    halo = send(pooled_v.at[pl.ds(T + B - 16, 16), :], halo_v, hs_sem, hr_sem, next_dev)

    @pl.when(jnp.logical_not(is_last))
    def _():
        halo.start()

    second[3].wait()

    def query_dots(c):
        q = gate_v[tile(c), :] + dot(x_v[tile(c), H : 2 * H], wq_v[H : 2 * H, :])
        q = q.astype(BF16).astype(F32)
        up = (silu(q) * explog_v[tile(c), :]).astype(BF16)
        for s in range(R // B):
            rows = pl.ds(c * R + s * B, B)
            for h in range(NH):
                hs = slice(h * DK, (h + 1) * DK)
                u = up[s * B : (s + 1) * B, hs]
                sc = dot_nt(u, down_v[rows, hs])
                sq_v[rows, 2 * h * DK : (2 * h + 1) * DK] = jnp.where(lower, sc, 0.0).astype(BF16)
                sq_v[rows, (2 * h + 1) * DK : (2 * h + 2) * DK] = u

    for c in range(NT):
        query_dots(c)

    s1_recv[x] = s1_send[x]
    for d in range(1, NX):
        arrival1(d).wait_recv()
    run = jnp.zeros((DK, DK), F32)
    logs = jnp.zeros((1, DK), F32)
    for k in range(NX):
        pre_v[k] = run
        bsum_v[k] = jnp.broadcast_to(logs, (8, DK))
        a_k = joined_rows(s1_recv[k, pl.ds(DK, 16), :])
        run = jnp.exp2(a_k) * run + s1_recv[k, pl.ds(0, DK), :].astype(F32)
        logs = logs + a_k
    s2_send[pl.ds(0, DK), :] = run.astype(BF16)
    s2_send[pl.ds(DK, 16), :] = split_rows(logs)

    def msg2(k):
        return send(s2_send, s2_recv.at[z], m2s_sem.at[k], m2r_sem.at[z], {"sp_0": k})

    for k in range(1, nz):

        @pl.when(k > z)
        def _():
            msg2(k).start()

    first[4].wait()
    second[4].wait()
    for k in range(2, 7):
        params[k].wait()

    def gate_dots(c):
        g = dot(x_v[tile(c), :], wg_v[...]).astype(BF16).astype(F32)
        gain = jnp.concatenate([rgain_v[...]] * NH, axis=1)
        gate_v[tile(c), :] = silu(g) * gain

    for c in range(NT):
        gate_dots(c)

    run_v[...] = jnp.zeros_like(run_v)
    for k in range(nz - 1):

        @pl.when(k < z)
        def _():
            send(s2_send, s2_recv.at[k], m2s_sem.at[k], m2r_sem.at[k], {"sp_0": k}).wait_recv()
            b_k = joined_rows(s2_recv[k, pl.ds(DK, 16), :])
            run_v[...] = jnp.exp2(b_k) * run_v[...] + s2_recv[k, pl.ds(0, DK), :].astype(F32)

    run = run_v[...]
    for k in range(NX):
        s3_send[k] = (jnp.exp2(bsum_v[k][0:1, :]) * run + pre_v[k]).astype(BF16)

    def msg3(d):
        to = lax.rem(x + d, NX)
        return send(s3_send.at[to], s3_recv.at[x], m3s_sem.at[d - 1], m3r_sem.at[x], {"sp_1": to})

    def arrival3(d):
        frm = lax.rem(x + d, NX)
        return send(s3_send.at[frm], s3_recv.at[frm], m3s_sem.at[d - 1], m3r_sem.at[frm], {"sp_1": frm})

    for d in range(1, NX):
        msg3(d).start()

    @pl.when(jnp.logical_not(is_first))
    def _():
        halo.wait_recv()
        pooled_v[pl.ds(B - 16, 16), :] = halo_v[...]

    pool_sends = [
        send(a_v.at[tile(c), pl.ds(0, C)], a_v.at[tile(c), pl.ds(C, C)], ps_sem.at[c], pr_sem.at[c], partner)
        for c in range(NT)
    ]

    def pooling(b):
        position = sp * T + b * B + lax.broadcasted_iota(jnp.int32, (B, 1), 0) + 1
        for g in range(2):
            cols = slice(g * 256, (g + 1) * 256)
            total = dot(band_v[g], pooled_v[pl.ds(b * B, 2 * B), cols])
            here = pooled_v[pl.ds((b + 1) * B, B), cols].astype(F32)
            width = jnp.left_shift(2, 2 * tp + g)
            if b == 0:
                diff = total / jnp.minimum(position, width).astype(F32) - here
            else:
                diff = total * (1.0 / width.astype(F32)) - here
            mixed = dot(diff.astype(BF16), pmix_v[g]) * pscale_v[:, cols]
            a_v[pl.ds(b * B, B), cols] = mixed.astype(BF16)

    for c in range(NT):
        for s in range(R // B):
            pooling(c * (R // B) + s)
        pool_sends[c].start()

    for c in out_loads:
        c.wait()
    for c in w_sends:
        c.wait_recv()
    def pool_project(c):
        pool_sends[c].wait_recv()
        resid_v[tile(c), :] = ALPHA * x_v[tile(c), 0:H].astype(F32) + dot(
            a_v[tile(c), 0 : 2 * C], wo_v[0 : 2 * C, :]
        )

    for c in range(NT - 1):
        pool_project(c)

    s3_recv[x] = s3_send[x]
    for d in range(1, NX):
        arrival3(d).wait_recv()

    rec_sends = [
        send(
            a_v.at[tile(c), pl.ds(2 * C, C)], a_v.at[tile(c), pl.ds(3 * C, C)],
            rs_sem.at[c], rr_sem.at[c], partner,
        )
        for c in range(NT)
    ]
    stat_sends = [
        send(stat_v.at[tile(c), :], ostat_v.at[tile(c), :], ss_sem.at[c], sr_sem.at[c], partner)
        for c in range(NT)
    ]

    def recur(b):
        rows = pl.ds(b * B, B)
        far = jnp.exp2(off_v[b])
        for h in range(NH):
            hs = slice(h * DK, (h + 1) * DK)
            state = st_v[b, h] + far[:, hs] * s3_recv[h].astype(F32)
            raw = dot(sq_v[rows, 2 * h * DK : (2 * h + 1) * DK], v_v[rows, hs])
            raw = raw + dot_nt(sq_v[rows, (2 * h + 1) * DK : (2 * h + 2) * DK], state.astype(BF16))
            power = jnp.mean(raw * raw, axis=1, keepdims=True)
            normed = raw * lax.rsqrt(power + EPS_RMS) * gate_v[rows, hs]
            a_v[rows, 2 * C + h * DK : 2 * C + (h + 1) * DK] = normed.astype(BF16)

    def project(c):
        resid = resid_v[tile(c), :] + dot(a_v[tile(c), 2 * C : 4 * C], wo_v[2 * C : 4 * C, :])
        resid_v[tile(c), :] = resid
        mean = jnp.sum(resid, axis=1, keepdims=True) * (1.0 / H)
        dev = resid - mean
        m2 = jnp.sum(dev * dev, axis=1, keepdims=True)
        lane = lax.broadcasted_iota(jnp.int32, (R, DK), 1)
        stat_v[tile(c), :] = jnp.where(lane == 0, mean, m2)

    def norm(c):
        mine = stat_v[tile(c), :]
        theirs = ostat_v[tile(c), :]
        gap = mine[:, 0:1] - theirs[:, 0:1]
        mean = 0.5 * (mine[:, 0:1] + theirs[:, 0:1])
        var = (mine[:, 1:2] + theirs[:, 1:2] + gap * gap * (0.5 * H)) * (1.0 / (2 * H))
        scale = lax.rsqrt(var + EPS_NORM)
        out[tile(c), :] = (
            (resid_v[tile(c), :] - mean) * scale * ngain_v[...] + nbias_v[...]
        ).astype(BF16)

    def recur_tile(c):
        for k in range(R // B):
            recur(c * (R // B) + k)
        rec_sends[c].start()

    recur_tile(0)
    pool_project(NT - 1)
    recur_tile(1)
    for c in range(NT):
        rec_sends[c].wait_recv()
        if c + 2 < NT:
            for k in range(R // B):
                recur((c + 2) * (R // B) + k)
        project(c)
        if c + 2 < NT:
            rec_sends[c + 2].start()
        stat_sends[c].start()
    for c in range(NT):
        stat_sends[c].wait_recv()
        norm(c)

    for c in range(NT):
        x_sends[c].wait_send()
        pool_sends[c].wait_send()
        rec_sends[c].wait_send()
        stat_sends[c].wait_send()
    for c in w_sends:
        c.wait_send()

    @pl.when(jnp.logical_not(is_last))
    def _():
        halo.wait_send()

    for d in range(1, NX):
        msg1(d).wait_send()
        msg3(d).wait_send()
    for k in range(1, nz):

        @pl.when(k > z)
        def _():
            msg2(k).wait_send()


def layer(nz, *args):
    (stream, wp, wq, wf, wv, wg, pmix, pscale, lb, ed, rgain, wop, wor, ngain, nbias) = args
    sem = pltpu.SemaphoreType.DMA
    scratch = [
        pltpu.VMEM((T, 2 * H), BF16),
        *[pltpu.VMEM((2 * H, C), BF16)] * 5,
        pltpu.VMEM((4 * C, H), BF16),
        pltpu.VMEM((2, 256, 256), BF16),
        pltpu.VMEM((1, C), F32),
        pltpu.VMEM((1, C), F32),
        pltpu.VMEM((NH, T), F32),
        pltpu.VMEM((T, NH), F32),
        pltpu.VMEM((1, DK), F32),
        pltpu.VMEM((1, H), F32),
        pltpu.VMEM((1, H), F32),
        pltpu.VMEM((T, C), F32),
        pltpu.VMEM((T, C), BF16),
        pltpu.VMEM((T, C), F32),
        pltpu.VMEM((T, C), BF16),
        pltpu.VMEM((T + B, C), BF16),
        pltpu.VMEM((16, C), BF16),
        pltpu.VMEM((T, 2 * C), BF16),
        pltpu.VMEM((T, C), F32),
        pltpu.VMEM((T, 4 * C), BF16),
        pltpu.VMEM((NB, NH, DK, DK), F32),
        pltpu.VMEM((NH, DK, DK), F32),
        pltpu.VMEM((NB, 1, C), F32),
        pltpu.VMEM((1, C), F32),
        pltpu.VMEM((2, B, 2 * B), BF16),
        pltpu.VMEM((B, 2 * B), BF16),
        pltpu.VMEM((NH, MSG, DK), BF16),
        pltpu.VMEM((NX, MSG, DK), BF16),
        pltpu.VMEM((MSG, DK), BF16),
        pltpu.VMEM((nz, MSG, DK), BF16),
        pltpu.VMEM((NX, DK, DK), BF16),
        pltpu.VMEM((NX, DK, DK), BF16),
        pltpu.VMEM((NX, DK, DK), F32),
        pltpu.VMEM((NX, 8, DK), F32),
        pltpu.VMEM((DK, DK), F32),
        pltpu.VMEM((T, H), F32),
        pltpu.VMEM((T, DK), F32),
        pltpu.VMEM((T, DK), F32),
        sem((NT + 12,)), sem((7,)),
        sem((NT,)), sem((NT,)), sem((2,)), sem((2,)), sem((NT,)), sem((NT,)),
        sem((NT,)), sem((NT,)), sem((NT,)), sem((NT,)),
        sem, sem,
        sem((NX - 1,)), sem((NX,)), sem((nz,)), sem((nz,)), sem((NX - 1,)), sem((NX,)),
    ]
    operands = (
        stream[0], wp, wq, wf, wv, wg, pmix,
        pscale.reshape(1, C), lb.reshape(1, C), ed.T, rgain.reshape(1, DK),
        wop, wor, ngain.reshape(1, H), nbias.reshape(1, H),
    )
    result = pl.pallas_call(
        functools.partial(kernel, nz),
        out_shape=pltpu.VMEM((T, H), BF16),
        in_specs=[pl.BlockSpec(memory_space=pltpu.HBM)] * 15,
        out_specs=pl.BlockSpec(memory_space=pltpu.VMEM),
        scratch_shapes=scratch,
        compiler_params=pltpu.CompilerParams(
            collective_id=0, has_side_effects=True, vmem_limit_bytes=58_000_000
        ),
    )(*[pltpu.with_memory_space_constraint(a, pltpu.HBM) for a in operands])
    return result[None]


def solution(mesh):
    devices = mesh.devices
    nz = devices.shape[0] // NX
    torus = Mesh(
        devices.reshape(nz, NX, mesh.shape["fs"], mesh.shape["tp"]), ("sp_0", "sp_1", "fs", "tp")
    )
    sp = ("sp_0", "sp_1")
    cols = P(None, "tp")
    return jax.shard_map(
        functools.partial(layer, nz),
        mesh=torus,
        in_specs=(
            P("fs", sp, "tp"), cols, cols, cols, cols, cols,
            P("tp", None, None), P("tp"), P("tp"), P(sp, "tp"), P(),
            P("tp", None), P("tp", None), P("tp"), P("tp"),
        ),
        out_specs=P("fs", sp, "tp"),
        check_vma=False,
    )
```

```python
import functools
import math

import jax
import jax.numpy as jnp
from jax import lax
from jax.experimental import pallas as pl
from jax.experimental.pallas import tpu as pltpu
from jax.sharding import Mesh
from jax.sharding import PartitionSpec as P

BF16 = jnp.bfloat16
F32 = jnp.float32
MESH = pl.DeviceIdType.MESH

ALPHA = 2.0**0.25
EPS_RMS = 1e-06
EPS_NORM = 1e-05
LOG2E = math.log2(math.e)

T = 1024
H = 1024
C = 512
DK = 128
NH = C // DK
B = 128
NB = T // B
R = 256
NT = T // R
RB = 512
NB_BIG = T // RB
NX = 4
MSG = DK + 16


def dot(a, b):
    return jnp.dot(a, b, preferred_element_type=F32)


def dot_tn(a, b):
    return lax.dot_general(a, b, (((0,), (0,)), ((), ())), preferred_element_type=F32)


def dot_nt(a, b):
    return lax.dot_general(a, b, (((1,), (1,)), ((), ())), preferred_element_type=F32)


def silu(x):
    half = 0.5 * x
    return half + half * jnp.tanh(half)


def split_rows(row):
    hi = row.astype(BF16)
    rest = row - hi.astype(F32)
    mid = rest.astype(BF16)
    low = (rest - mid.astype(F32)).astype(BF16)
    rows = lax.broadcasted_iota(jnp.int32, (16, DK), 0)
    return jnp.where(
        rows == 0,
        hi.astype(F32),
        jnp.where(rows == 1, mid.astype(F32), jnp.where(rows == 2, low.astype(F32), 0.0)),
    ).astype(BF16)


def joined_rows(block):
    return jnp.sum(block.astype(F32), axis=0, keepdims=True)


def kernel(
    nz,
    stream, wp, wq, wf, wv, wg, pmix, pscale, lbound, edecay, rgain, wop, wor, ngain, nbias,
    out,
    x_v, wf_v, wv_v, wp_v, wq_v, wg_v, wo_v,
    pmix_v, pscale_v, lb_v, ed_v, edc_v, rgain_v, ngain_v, nbias_v,
    f_v, v_v, explog_v, down_v, pooled_v, halo_v, sq_v, gate_v, a_v,
    st_v, cur_v, off_v, offcur_v, band_v, tri_v,
    s1_send, s1_recv, s2_send, s2_recv, s3_send, s3_recv, pre_v, bsum_v, run_v,
    resid_v, stat_v, ostat_v,
    load_sem, param_sem,
    xs_sem, xr_sem, ws_sem, wr_sem, ps_sem, pr_sem, rs_sem, rr_sem, ss_sem, sr_sem,
    hs_sem, hr_sem, m1s_sem, m1r_sem, m2s_sem, m2r_sem, m3s_sem, m3r_sem,
):
    z = lax.axis_index("sp_0")
    x = lax.axis_index("sp_1")
    tp = lax.axis_index("tp")
    sp = z * NX + x
    other = 1 - tp
    n_sp = nz * NX
    after = lax.rem(sp + 1, n_sp)
    prior = lax.rem(sp + n_sp - 1, n_sp)
    is_first, is_last = sp == 0, sp == n_sp - 1
    partner = {"tp": other}
    x_peers = [{"sp_1": lax.rem(x + d, NX)} for d in range(1, NX)]
    z_peers = [{"sp_0": lax.rem(z + d, nz)} for d in range(1, nz)]
    next_dev = {"sp_0": after // NX, "sp_1": lax.rem(after, NX)}
    prev_dev = {"sp_0": prior // NX, "sp_1": lax.rem(prior, NX)}

    barrier = pltpu.get_barrier_semaphore()
    greeted = [partner] + x_peers + z_peers
    for dev in greeted:
        pl.semaphore_signal(barrier, inc=1, device_id=dev, device_id_type=MESH)

    @pl.when(jnp.logical_not(is_last))
    def _():
        pl.semaphore_signal(barrier, inc=1, device_id=next_dev, device_id_type=MESH)

    @pl.when(jnp.logical_not(is_first))
    def _():
        pl.semaphore_signal(barrier, inc=1, device_id=prev_dev, device_id_type=MESH)


    own_half = pl.ds(pl.multiple_of(tp * H, H), H)
    oth_half = pl.ds(pl.multiple_of(other * H, H), H)

    def tile(c):
        return pl.ds(c * R, R)

    def big(c):
        return pl.ds(c * RB, RB)

    loads = [
        pltpu.make_async_copy(stream.at[tile(c), :], x_v.at[tile(c), pl.ds(0, H)], load_sem.at[c])
        for c in range(NT)
    ]
    first, second = {}, {}
    for k, (src, dst) in enumerate(((wf, wf_v), (wv, wv_v), (wp, wp_v), (wq, wq_v), (wg, wg_v))):
        first[k] = pltpu.make_async_copy(
            src.at[own_half, :], dst.at[pl.ds(0, H), :], load_sem.at[NT + 2 * k]
        )
        second[k] = pltpu.make_async_copy(
            src.at[oth_half, :], dst.at[pl.ds(H, H), :], load_sem.at[NT + 2 * k + 1]
        )
    params = [
        pltpu.make_async_copy(src, dst, param_sem.at[k])
        for k, (src, dst) in enumerate(
            (
                (lbound, lb_v), (edecay, ed_v), (pmix, pmix_v), (pscale, pscale_v),
                (rgain, rgain_v), (ngain, ngain_v), (nbias, nbias_v),
            )
        )
    ]
    out_loads = [
        pltpu.make_async_copy(
            src.at[:, own_half], wo_v.at[pl.ds(2 * k * C, C), :], load_sem.at[NT + 10 + k]
        )
        for k, src in enumerate((wop, wor))
    ]
    def start_x(c):
        for k in range(2):
            rows = pl.ds(c * R + k * (R // 2), R // 2)
            pltpu.make_async_copy(stream.at[rows, :], x_v.at[rows, pl.ds(0, H)], load_sem.at[c]).start()

    start_x(0)
    for k in range(4):
        pltpu.make_async_copy(
            wf.at[pl.ds(pl.multiple_of(tp * H + k * 256, 256), 256), :],
            wf_v.at[pl.ds(k * 256, 256), :],
            load_sem.at[NT],
        ).start()
    for c in range(1, NT):
        start_x(c)
    first[1].start()
    for k in range(7):
        params[k].start()

    row = lax.broadcasted_iota(jnp.int32, (B, B), 0)
    col = lax.broadcasted_iota(jnp.int32, (B, B), 1)
    lower = row >= col
    ones = jnp.where(lower, 1.0, 0.0).astype(BF16)
    tri_v[:, 0:B] = ones
    tri_v[:, B : 2 * B] = ones
    brow = lax.broadcasted_iota(jnp.int32, (B, 2 * B), 0)
    lag = brow + B - lax.broadcasted_iota(jnp.int32, (B, 2 * B), 1)
    for g in range(2):
        width = jnp.left_shift(2, 2 * tp + g)
        band_v[g] = jnp.where((lag >= 0) & (lag < width), 1.0, 0.0).astype(BF16)
    cur_v[...] = jnp.zeros_like(cur_v)
    offcur_v[...] = jnp.zeros_like(offcur_v)
    pooled_v[pl.ds(0, B), :] = jnp.zeros((B, C), BF16)

    first[0].wait()
    for c in range(NT):
        loads[c].wait()
        f_v[tile(c), :] = dot(x_v[tile(c), 0:H], wf_v[0:H, :])

    for k in (2, 3):
        first[k].start()
    for k in (0, 1, 2, 3):
        second[k].start()

    first[1].wait()
    for c in range(NB_BIG):
        resid_v[big(c), 0:C] = dot(x_v[big(c), 0:H], wv_v[0:H, :])
    pl.semaphore_wait(barrier, len(greeted) + jnp.minimum(sp, 1) + jnp.minimum(n_sp - 1 - sp, 1))

    def send(src, dst, s_sem, r_sem, dev):
        return pltpu.make_async_remote_copy(
            src_ref=src, dst_ref=dst, send_sem=s_sem, recv_sem=r_sem, device_id=dev, device_id_type=MESH
        )

    x_sends = [
        send(
            x_v.at[tile(c), pl.ds(0, H)], x_v.at[tile(c), pl.ds(H, H)],
            xs_sem.at[c], xr_sem.at[c], partner,
        )
        for c in range(NT)
    ]
    for c in x_sends:
        c.start()
    w_sends = [
        send(
            src.at[:, oth_half], wo_v.at[pl.ds((2 * k + 1) * C, C), :], ws_sem.at[k], wr_sem.at[k], partner
        )
        for k, src in enumerate((wop, wor))
    ]

    first[2].wait()
    for c in range(NB_BIG):
        resid_v[big(c), C : 2 * C] = dot(x_v[big(c), 0:H], wp_v[0:H, :])
    first[4].start()
    second[4].start()
    for c in out_loads:
        c.start()
    first[3].wait()
    for c in range(NB_BIG):
        gate_v[big(c), :] = dot(x_v[big(c), 0:H], wq_v[0:H, :])
    params[0].wait()
    params[1].wait()
    for b in range(NB):
        edc_v[pl.ds(b * B, B), :] = jnp.transpose(ed_v[:, b * B : (b + 1) * B] * LOG2E)

    def forget_dots(c):
        f_v[tile(c), :] = f_v[tile(c), :] + dot(x_v[tile(c), H : 2 * H], wf_v[H : 2 * H, :])
        v_v[tile(c), :] = (
            resid_v[tile(c), 0:C] + dot(x_v[tile(c), H : 2 * H], wv_v[H : 2 * H, :])
        ).astype(BF16)

    def pooled_dots(c):
        pooled_v[pl.ds(c * RB + B, RB), :] = (
            resid_v[big(c), C : 2 * C] + dot(x_v[big(c), H : 2 * H], wp_v[H : 2 * H, :])
        ).astype(BF16)

    def forget_block(b):
        rows = pl.ds(b * B, B)
        ed = edc_v[rows, :]
        off = offcur_v[...]
        off_v[b] = off
        for p in range(NH // 2):
            cols = slice(2 * p * DK, 2 * (p + 1) * DK)
            half_gap = 0.5 - 0.5 * lb_v[:, cols]
            w_in = half_gap - half_gap * jnp.tanh(0.5 * f_v[rows, cols])
            keep = jnp.log(1.0 - w_in) * LOG2E
            keep = jnp.concatenate(
                [keep[:, k * DK : (k + 1) * DK] + ed[:, 2 * p + k : 2 * p + k + 1] for k in range(2)], axis=1
            )
            hi = keep.astype(BF16)
            lo = (keep - hi.astype(F32)).astype(BF16)
            total = dot(tri_v[...], jnp.concatenate([hi, lo], axis=0))
            end = total[B - 1 : B, :]
            explog_v[rows, cols] = jnp.exp2(total)
            down_v[rows, cols] = (w_in * jnp.exp2(-total)).astype(BF16)
            inw = (w_in * jnp.exp2(end - total)).astype(BF16)
            kept = jnp.exp2(end)
            offcur_v[:, cols] = off[:, cols] + end
            for k in range(2):
                h = 2 * p + k
                hs = slice(k * DK, (k + 1) * DK)
                st = cur_v[h]
                st_v[b, h] = st
                cur_v[h] = kept[:, hs] * st + dot_tn(v_v[rows, h * DK : (h + 1) * DK], inw[:, hs])

    second[0].wait()
    second[1].wait()
    x_sends[0].wait_recv()
    forget_dots(0)
    second[2].wait()
    for c in range(NT):
        if c + 1 < NT:
            x_sends[c + 1].wait_recv()
            forget_dots(c + 1)
        else:
            pooled_dots(0)
        for s in range(R // B):
            forget_block(c * (R // B) + s)

    for h in range(NH):
        s1_send[h, pl.ds(0, DK), :] = cur_v[h].astype(BF16)
        s1_send[h, pl.ds(DK, 16), :] = split_rows(offcur_v[0:1, h * DK : (h + 1) * DK])

    def msg1(d):
        to = lax.rem(x + d, NX)
        return send(s1_send.at[to], s1_recv.at[x], m1s_sem.at[d - 1], m1r_sem.at[x], {"sp_1": to})

    def arrival1(d):
        frm = lax.rem(x + d, NX)
        return send(s1_send.at[frm], s1_recv.at[frm], m1s_sem.at[d - 1], m1r_sem.at[frm], {"sp_1": frm})

    for d in (2, 1, 3):
        msg1(d).start()
    for c in w_sends:
        c.start()

    pooled_dots(1)

    halo = send(pooled_v.at[pl.ds(T + B - 16, 16), :], halo_v, hs_sem, hr_sem, next_dev)

    @pl.when(jnp.logical_not(is_last))
    def _():
        halo.start()

    second[3].wait()

    def query_dots(c):
        q = gate_v[tile(c), :] + dot(x_v[tile(c), H : 2 * H], wq_v[H : 2 * H, :])
        up = (silu(q) * explog_v[tile(c), :]).astype(BF16)
        for s in range(R // B):
            rows = pl.ds(c * R + s * B, B)
            for h in range(NH):
                hs = slice(h * DK, (h + 1) * DK)
                u = up[s * B : (s + 1) * B, hs]
                sc = dot_nt(u, down_v[rows, hs])
                sq_v[rows, 2 * h * DK : (2 * h + 1) * DK] = jnp.where(lower, sc, 0.0).astype(BF16)
                sq_v[rows, (2 * h + 1) * DK : (2 * h + 2) * DK] = u

    for c in range(NT):
        query_dots(c)

    def msg2(k):
        return send(s2_send, s2_recv.at[z], m2s_sem.at[k], m2r_sem.at[z], {"sp_0": k})

    def msg3(d):
        to = lax.rem(x + d, NX)
        return send(s3_send.at[to], s3_recv.at[x], m3s_sem.at[d - 1], m3r_sem.at[x], {"sp_1": to})

    def arrival3(d):
        frm = lax.rem(x + d, NX)
        return send(s3_send.at[frm], s3_recv.at[frm], m3s_sem.at[d - 1], m3r_sem.at[frm], {"sp_1": frm})

    def row_prefix():
        s1_recv[x] = s1_send[x]
        for d in range(1, NX):
            arrival1(d).wait_recv()
        run = jnp.zeros((DK, DK), F32)
        logs = jnp.zeros((1, DK), F32)
        for k in range(NX):
            pre_v[k] = run
            bsum_v[k] = jnp.broadcast_to(logs, (8, DK))
            a_k = joined_rows(s1_recv[k, pl.ds(DK, 16), :])
            run = jnp.exp2(a_k) * run + s1_recv[k, pl.ds(0, DK), :].astype(F32)
            logs = logs + a_k
        s2_send[pl.ds(0, DK), :] = run.astype(BF16)
        s2_send[pl.ds(DK, 16), :] = split_rows(logs)

        for k in range(1, nz):

            @pl.when(k > z)
            def _():
                msg2(k).start()

    def column_prefix():
        run_v[...] = jnp.zeros_like(run_v)
        for k in range(nz - 1):

            @pl.when(k < z)
            def _():
                send(s2_send, s2_recv.at[k], m2s_sem.at[k], m2r_sem.at[k], {"sp_0": k}).wait_recv()
                b_k = joined_rows(s2_recv[k, pl.ds(DK, 16), :])
                run_v[...] = jnp.exp2(b_k) * run_v[...] + s2_recv[k, pl.ds(0, DK), :].astype(F32)

        run = run_v[...]
        for k in range(NX):
            s3_send[k] = (jnp.exp2(bsum_v[k][0:1, :]) * run + pre_v[k]).astype(BF16)

        for d in (2, 1, 3):
            msg3(d).start()

    @pl.when(x > 0)
    def _():
        row_prefix()

        @pl.when(z == 0)
        def _():
            column_prefix()

    first[4].wait()
    second[4].wait()
    for k in range(2, 7):
        params[k].wait()

    def gate_dots(c):
        g = dot(x_v[tile(c), :], wg_v[...])
        gain = jnp.concatenate([rgain_v[...]] * NH, axis=1)
        gate_v[tile(c), :] = silu(g) * gain

    pool_sends = [
        send(a_v.at[tile(c), pl.ds(0, C)], a_v.at[tile(c), pl.ds(C, C)], ps_sem.at[c], pr_sem.at[c], partner)
        for c in range(NT)
    ]

    def pooling(b):
        position = sp * T + b * B + lax.broadcasted_iota(jnp.int32, (B, 1), 0) + 1
        for g in range(2):
            cols = slice(g * 256, (g + 1) * 256)
            total = dot(band_v[g], pooled_v[pl.ds(b * B, 2 * B), cols])
            here = pooled_v[pl.ds((b + 1) * B, B), cols].astype(F32)
            width = jnp.left_shift(2, 2 * tp + g)
            if b == 0:
                diff = total / jnp.minimum(position, width).astype(F32) - here
            else:
                diff = total * (1.0 / width.astype(F32)) - here
            mixed = dot(diff.astype(BF16), pmix_v[g]) * pscale_v[:, cols]
            a_v[pl.ds(b * B, B), cols] = mixed.astype(BF16)

    def pool_tiles(c):
        for k in range(R // B):
            pooling(c * (R // B) + k)

    gate_dots(0)
    gate_dots(1)
    pool_tiles(1)
    pool_sends[1].start()

    @pl.when(x == 0)
    def _():
        row_prefix()

        @pl.when(z == 0)
        def _():
            column_prefix()

    @pl.when((x > 0) & (z > 0))
    def _():
        column_prefix()

    gate_dots(2)
    pool_tiles(2)
    pool_sends[2].start()

    @pl.when((x == 0) & (z > 0))
    def _():
        column_prefix()

    @pl.when(jnp.logical_not(is_first))
    def _():
        halo.wait_recv()
        pooled_v[pl.ds(B - 16, 16), :] = halo_v[...]

    gate_dots(3)
    pool_tiles(3)
    pool_tiles(0)
    pool_sends[3].start()
    pool_sends[0].start()

    for c in out_loads:
        c.wait()
    for c in w_sends:
        c.wait_recv()
    def pool_project(c):
        resid_v[tile(c), :] = ALPHA * x_v[tile(c), 0:H].astype(F32) + dot(
            a_v[tile(c), 0 : 2 * C], wo_v[0 : 2 * C, :]
        )

    for c in range(1, NT):
        pool_sends[c].wait_recv()
        pool_project(c)

    s3_recv[x] = s3_send[x]
    for d in range(1, NX):
        arrival3(d).wait_recv()

    rec_sends = [
        send(
            a_v.at[tile(c), pl.ds(2 * C, C)], a_v.at[tile(c), pl.ds(3 * C, C)],
            rs_sem.at[c], rr_sem.at[c], partner,
        )
        for c in range(NT)
    ]
    stat_sends = [
        send(stat_v.at[tile(c), :], ostat_v.at[tile(c), :], ss_sem.at[c], sr_sem.at[c], partner)
        for c in range(NT)
    ]

    def recur(b):
        rows = pl.ds(b * B, B)
        far = jnp.exp2(off_v[b])
        for h in range(NH):
            hs = slice(h * DK, (h + 1) * DK)
            state = st_v[b, h] + far[:, hs] * s3_recv[h].astype(F32)
            raw = dot(sq_v[rows, 2 * h * DK : (2 * h + 1) * DK], v_v[rows, hs])
            raw = raw + dot_nt(sq_v[rows, (2 * h + 1) * DK : (2 * h + 2) * DK], state.astype(BF16))
            power = jnp.mean(raw * raw, axis=1, keepdims=True)
            normed = raw * lax.rsqrt(power + EPS_RMS) * gate_v[rows, hs]
            a_v[rows, 2 * C + h * DK : 2 * C + (h + 1) * DK] = normed.astype(BF16)

    def project(c):
        resid_v[tile(c), :] = resid_v[tile(c), :] + dot(
            a_v[tile(c), 2 * C : 4 * C], wo_v[2 * C : 4 * C, :]
        )

    def stats(c):
        resid = resid_v[tile(c), :]
        mean = jnp.sum(resid, axis=1, keepdims=True) * (1.0 / H)
        dev = resid - mean
        m2 = jnp.sum(dev * dev, axis=1, keepdims=True)
        lane = lax.broadcasted_iota(jnp.int32, (R, DK), 1)
        stat_v[tile(c), :] = jnp.where(lane == 0, mean, m2)

    def norm(c):
        mine = stat_v[tile(c), :]
        theirs = ostat_v[tile(c), :]
        gap = mine[:, 0:1] - theirs[:, 0:1]
        mean = 0.5 * (mine[:, 0:1] + theirs[:, 0:1])
        var = (mine[:, 1:2] + theirs[:, 1:2] + gap * gap * (0.5 * H)) * (1.0 / (2 * H))
        scale = lax.rsqrt(var + EPS_NORM)
        out[tile(c), :] = (
            (resid_v[tile(c), :] - mean) * scale * ngain_v[...] + nbias_v[...]
        ).astype(BF16)

    def recur_tile(c):
        for k in range(R // B):
            recur(c * (R // B) + k)
        rec_sends[c].start()

    recur_tile(0)
    pool_sends[0].wait_recv()
    for k in range(R // B, 3 * R // B):
        recur(k)
    pool_project(0)
    rec_sends[1].start()
    rec_sends[2].start()
    rec_sends[0].wait_recv()
    for k in range(3 * R // B, T // B):
        recur(k)
    project(0)
    rec_sends[3].start()
    for c in range(1, NT):
        rec_sends[c].wait_recv()
        project(c)
        stats(c - 1)
        stat_sends[c - 1].start()
    stats(NT - 1)
    stat_sends[NT - 1].start()
    for c in range(NT):
        stat_sends[c].wait_recv()
        norm(c)

    for c in range(NT):
        x_sends[c].wait_send()
        pool_sends[c].wait_send()
        rec_sends[c].wait_send()
        stat_sends[c].wait_send()
    for c in w_sends:
        c.wait_send()

    @pl.when(jnp.logical_not(is_last))
    def _():
        halo.wait_send()

    for d in range(1, NX):
        msg1(d).wait_send()
        msg3(d).wait_send()
    for k in range(1, nz):

        @pl.when(k > z)
        def _():
            msg2(k).wait_send()


def layer(nz, *args):
    (stream, wp, wq, wf, wv, wg, pmix, pscale, lb, ed, rgain, wop, wor, ngain, nbias) = args
    sem = pltpu.SemaphoreType.DMA
    scratch = [
        pltpu.VMEM((T, 2 * H), BF16),
        *[pltpu.VMEM((2 * H, C), BF16)] * 5,
        pltpu.VMEM((4 * C, H), BF16),
        pltpu.VMEM((2, 256, 256), BF16),
        pltpu.VMEM((1, C), F32),
        pltpu.VMEM((1, C), F32),
        pltpu.VMEM((NH, T), F32),
        pltpu.VMEM((T, NH), F32),
        pltpu.VMEM((1, DK), F32),
        pltpu.VMEM((1, H), F32),
        pltpu.VMEM((1, H), F32),
        pltpu.VMEM((T, C), F32),
        pltpu.VMEM((T, C), BF16),
        pltpu.VMEM((T, C), F32),
        pltpu.VMEM((T, C), BF16),
        pltpu.VMEM((T + B, C), BF16),
        pltpu.VMEM((16, C), BF16),
        pltpu.VMEM((T, 2 * C), BF16),
        pltpu.VMEM((T, C), F32),
        pltpu.VMEM((T, 4 * C), BF16),
        pltpu.VMEM((NB, NH, DK, DK), F32),
        pltpu.VMEM((NH, DK, DK), F32),
        pltpu.VMEM((NB, 1, C), F32),
        pltpu.VMEM((1, C), F32),
        pltpu.VMEM((2, B, 2 * B), BF16),
        pltpu.VMEM((B, 2 * B), BF16),
        pltpu.VMEM((NH, MSG, DK), BF16),
        pltpu.VMEM((NX, MSG, DK), BF16),
        pltpu.VMEM((MSG, DK), BF16),
        pltpu.VMEM((nz, MSG, DK), BF16),
        pltpu.VMEM((NX, DK, DK), BF16),
        pltpu.VMEM((NX, DK, DK), BF16),
        pltpu.VMEM((NX, DK, DK), F32),
        pltpu.VMEM((NX, 8, DK), F32),
        pltpu.VMEM((DK, DK), F32),
        pltpu.VMEM((T, H), F32),
        pltpu.VMEM((T, DK), F32),
        pltpu.VMEM((T, DK), F32),
        sem((NT + 12,)), sem((7,)),
        sem((NT,)), sem((NT,)), sem((2,)), sem((2,)), sem((NT,)), sem((NT,)),
        sem((NT,)), sem((NT,)), sem((NT,)), sem((NT,)),
        sem, sem,
        sem((NX - 1,)), sem((NX,)), sem((nz,)), sem((nz,)), sem((NX - 1,)), sem((NX,)),
    ]
    operands = (
        stream[0], wp, wq, wf, wv, wg, pmix,
        pscale.reshape(1, C), lb.reshape(1, C), ed.T, rgain.reshape(1, DK),
        wop, wor, ngain.reshape(1, H), nbias.reshape(1, H),
    )
    result = pl.pallas_call(
        functools.partial(kernel, nz),
        out_shape=pltpu.VMEM((T, H), BF16),
        in_specs=[pl.BlockSpec(memory_space=pltpu.HBM)] * 15,
        out_specs=pl.BlockSpec(memory_space=pltpu.VMEM),
        scratch_shapes=scratch,
        compiler_params=pltpu.CompilerParams(
            collective_id=0, has_side_effects=True, vmem_limit_bytes=58_000_000
        ),
    )(*[pltpu.with_memory_space_constraint(a, pltpu.HBM) for a in operands])
    return result[None]


def solution(mesh):
    devices = mesh.devices
    nz = devices.shape[0] // NX
    torus = Mesh(
        devices.reshape(nz, NX, mesh.shape["fs"], mesh.shape["tp"]), ("sp_0", "sp_1", "fs", "tp")
    )
    sp = ("sp_0", "sp_1")
    cols = P(None, "tp")
    return jax.shard_map(
        functools.partial(layer, nz),
        mesh=torus,
        in_specs=(
            P("fs", sp, "tp"), cols, cols, cols, cols, cols,
            P("tp", None, None), P("tp"), P("tp"), P(sp, "tp"), P(),
            P("tp", None), P("tp", None), P("tp"), P("tp"),
        ),
        out_specs=P("fs", sp, "tp"),
        check_vma=False,
    )
```

```python
import functools
import math

import jax
import jax.numpy as jnp
from jax import lax
from jax.experimental import pallas as pl
from jax.experimental.pallas import tpu as pltpu
from jax.sharding import Mesh
from jax.sharding import PartitionSpec as P

BF16 = jnp.bfloat16
F32 = jnp.float32
MESH = pl.DeviceIdType.MESH

ALPHA = 2.0**0.25
EPS_RMS = 1e-06
EPS_NORM = 1e-05
LOG2E = math.log2(math.e)

T = 1024
H = 1024
C = 512
DK = 128
NH = C // DK
B = 128
NB = T // B
R = 256
NT = T // R
RB = 512
NB_BIG = T // RB
NX = 4
MSG = DK + 16


def dot(a, b):
    return jnp.dot(a, b, preferred_element_type=F32)


def dot_tn(a, b):
    return lax.dot_general(a, b, (((0,), (0,)), ((), ())), preferred_element_type=F32)


def dot_nt(a, b):
    return lax.dot_general(a, b, (((1,), (1,)), ((), ())), preferred_element_type=F32)


def silu(x):
    half = 0.5 * x
    return half + half * jnp.tanh(half)


def split_rows(row):
    hi = row.astype(BF16)
    rest = row - hi.astype(F32)
    mid = rest.astype(BF16)
    low = (rest - mid.astype(F32)).astype(BF16)
    rows = lax.broadcasted_iota(jnp.int32, (16, DK), 0)
    return jnp.where(
        rows == 0,
        hi.astype(F32),
        jnp.where(rows == 1, mid.astype(F32), jnp.where(rows == 2, low.astype(F32), 0.0)),
    ).astype(BF16)


def joined_rows(block):
    return jnp.sum(block.astype(F32), axis=0, keepdims=True)


def kernel(
    nz,
    stream, wp, wq, wf, wv, wg, pmix, pscale, lbound, edecay, rgain, wop, wor, ngain, nbias,
    out,
    x_v, wf_v, wv_v, wp_v, wq_v, wg_v, wo_v,
    pmix_v, pscale_v, lb_v, ed_v, edc_v, rgain_v, ngain_v, nbias_v,
    f_v, hl_v, inw_v, end_v, v_v, explog_v, down_v, pooled_v, halo_v, sq_v, gate_v, a_v,
    st_v, cur_v, off_v, offcur_v, band_v, tri_v,
    s1_send, s1_recv, s2_send, s2_recv, s3_send, s3_recv, pre_v, bsum_v, run_v,
    resid_v, stat_v, ostat_v,
    load_sem, param_sem,
    xs_sem, xr_sem, ws_sem, wr_sem, ps_sem, pr_sem, rs_sem, rr_sem, ss_sem, sr_sem,
    hs_sem, hr_sem, m1s_sem, m1r_sem, m2s_sem, m2r_sem, m3s_sem, m3r_sem,
):
    z = lax.axis_index("sp_0")
    x = lax.axis_index("sp_1")
    tp = lax.axis_index("tp")
    sp = z * NX + x
    other = 1 - tp
    n_sp = nz * NX
    after = lax.rem(sp + 1, n_sp)
    prior = lax.rem(sp + n_sp - 1, n_sp)
    is_first, is_last = sp == 0, sp == n_sp - 1
    partner = {"tp": other}
    x_peers = [{"sp_1": lax.rem(x + d, NX)} for d in range(1, NX)]
    z_peers = [{"sp_0": lax.rem(z + d, nz)} for d in range(1, nz)]
    next_dev = {"sp_0": after // NX, "sp_1": lax.rem(after, NX)}
    prev_dev = {"sp_0": prior // NX, "sp_1": lax.rem(prior, NX)}

    barrier = pltpu.get_barrier_semaphore()
    greeted = [partner] + x_peers + z_peers
    for dev in greeted:
        pl.semaphore_signal(barrier, inc=1, device_id=dev, device_id_type=MESH)

    @pl.when(jnp.logical_not(is_last))
    def _():
        pl.semaphore_signal(barrier, inc=1, device_id=next_dev, device_id_type=MESH)

    @pl.when(jnp.logical_not(is_first))
    def _():
        pl.semaphore_signal(barrier, inc=1, device_id=prev_dev, device_id_type=MESH)


    own_half = pl.ds(pl.multiple_of(tp * H, H), H)
    oth_half = pl.ds(pl.multiple_of(other * H, H), H)

    def tile(c):
        return pl.ds(c * R, R)

    def big(c):
        return pl.ds(c * RB, RB)

    loads = [
        pltpu.make_async_copy(stream.at[tile(c), :], x_v.at[tile(c), pl.ds(0, H)], load_sem.at[c])
        for c in range(NT)
    ]
    first, second = {}, {}
    for k, (src, dst) in enumerate(((wf, wf_v), (wv, wv_v), (wp, wp_v), (wq, wq_v), (wg, wg_v))):
        first[k] = pltpu.make_async_copy(
            src.at[own_half, :], dst.at[pl.ds(0, H), :], load_sem.at[NT + 2 * k]
        )
        second[k] = pltpu.make_async_copy(
            src.at[oth_half, :], dst.at[pl.ds(H, H), :], load_sem.at[NT + 2 * k + 1]
        )
    params = [
        pltpu.make_async_copy(src, dst, param_sem.at[k])
        for k, (src, dst) in enumerate(
            (
                (lbound, lb_v), (edecay, ed_v), (pmix, pmix_v), (pscale, pscale_v),
                (rgain, rgain_v), (ngain, ngain_v), (nbias, nbias_v),
            )
        )
    ]
    out_loads = [
        pltpu.make_async_copy(
            src.at[:, own_half], wo_v.at[pl.ds(2 * k * C, C), :], load_sem.at[NT + 10 + k]
        )
        for k, src in enumerate((wop, wor))
    ]
    def start_x(c):
        for k in range(2):
            rows = pl.ds(c * R + k * (R // 2), R // 2)
            pltpu.make_async_copy(stream.at[rows, :], x_v.at[rows, pl.ds(0, H)], load_sem.at[c]).start()

    start_x(0)
    for k in range(4):
        pltpu.make_async_copy(
            wf.at[pl.ds(pl.multiple_of(tp * H + k * 256, 256), 256), :],
            wf_v.at[pl.ds(k * 256, 256), :],
            load_sem.at[NT],
        ).start()
    for c in range(1, NT):
        start_x(c)

    row = lax.broadcasted_iota(jnp.int32, (B, B), 0)
    col = lax.broadcasted_iota(jnp.int32, (B, B), 1)
    lower = row >= col
    ones = jnp.where(lower, 1.0, 0.0).astype(BF16)
    tri_v[:, 0:B] = ones
    tri_v[:, B : 2 * B] = ones
    brow = lax.broadcasted_iota(jnp.int32, (B, 2 * B), 0)
    lag = brow + B - lax.broadcasted_iota(jnp.int32, (B, 2 * B), 1)
    for g in range(2):
        width = jnp.left_shift(2, 2 * tp + g)
        band_v[g] = jnp.where((lag >= 0) & (lag < width), 1.0, 0.0).astype(BF16)
    cur_v[...] = jnp.zeros_like(cur_v)
    offcur_v[...] = jnp.zeros_like(offcur_v)
    pooled_v[pl.ds(0, B), :] = jnp.zeros((B, C), BF16)

    first[0].wait()
    first[1].start()
    for k in range(7):
        params[k].start()
    for c in range(NT):
        loads[c].wait()
        f_v[tile(c), :] = dot(x_v[tile(c), 0:H], wf_v[0:H, :])

    first[2].start()
    for k in (0, 1, 2):
        second[k].start()

    first[1].wait()
    for c in range(NB_BIG):
        resid_v[big(c), 0:C] = dot(x_v[big(c), 0:H], wv_v[0:H, :])
    pl.semaphore_wait(barrier, len(greeted) + jnp.minimum(sp, 1) + jnp.minimum(n_sp - 1 - sp, 1))

    def send(src, dst, s_sem, r_sem, dev):
        return pltpu.make_async_remote_copy(
            src_ref=src, dst_ref=dst, send_sem=s_sem, recv_sem=r_sem, device_id=dev, device_id_type=MESH
        )

    x_sends = [
        send(
            x_v.at[tile(c), pl.ds(0, H)], x_v.at[tile(c), pl.ds(H, H)],
            xs_sem.at[c], xr_sem.at[c], partner,
        )
        for c in range(NT)
    ]
    for c in x_sends:
        c.start()
    w_sends = [
        send(
            src.at[:, oth_half], wo_v.at[pl.ds((2 * k + 1) * C, C), :], ws_sem.at[k], wr_sem.at[k], partner
        )
        for k, src in enumerate((wop, wor))
    ]

    first[2].wait()
    for c in range(NB_BIG):
        resid_v[big(c), C : 2 * C] = dot(x_v[big(c), 0:H], wp_v[0:H, :])
    for k in (3, 4):
        first[k].start()
        second[k].start()
    for c in out_loads:
        c.start()
    params[0].wait()
    params[1].wait()
    for b in range(NB):
        edc_v[pl.ds(b * B, B), :] = jnp.transpose(ed_v[:, b * B : (b + 1) * B] * LOG2E)

    def forget_dots(c):
        f_v[tile(c), :] = f_v[tile(c), :] + dot(x_v[tile(c), H : 2 * H], wf_v[H : 2 * H, :])

    def value_dots(c):
        v_v[tile(c), :] = (
            resid_v[tile(c), 0:C] + dot(x_v[tile(c), H : 2 * H], wv_v[H : 2 * H, :])
        ).astype(BF16)

    def pooled_dots(c):
        pooled_v[pl.ds(c * RB + B, RB), :] = (
            resid_v[big(c), C : 2 * C] + dot(x_v[big(c), H : 2 * H], wp_v[H : 2 * H, :])
        ).astype(BF16)

    def forget_gate(b):
        rows = pl.ds(b * B, B)
        ed = edc_v[rows, :]
        for h in range(NH):
            cols = slice(h * DK, (h + 1) * DK)
            half_gap = 0.5 - 0.5 * lb_v[:, cols]
            w_in = half_gap - half_gap * jnp.tanh(0.5 * f_v[rows, cols])
            f_v[rows, cols] = w_in
            keep = jnp.log(1.0 - w_in) * LOG2E + ed[:, h : h + 1]
            hi = keep.astype(BF16)
            hl_v[b % 4, 0:B, cols] = hi
            hl_v[b % 4, B : 2 * B, cols] = (keep - hi.astype(F32)).astype(BF16)

    def forget_sums(b):
        return [dot(tri_v[...], hl_v[b % 4, :, 2 * p * DK : 2 * (p + 1) * DK]) for p in range(NH // 2)]

    def forget_exps(b, sums):
        rows = pl.ds(b * B, B)
        off_v[b] = offcur_v[...]
        for p in range(NH // 2):
            cols = slice(2 * p * DK, 2 * (p + 1) * DK)
            total = sums[p]
            end = total[B - 1 : B, :]
            w_in = f_v[rows, cols]
            explog_v[rows, cols] = jnp.exp2(total)
            down_v[rows, cols] = (w_in * jnp.exp2(-total)).astype(BF16)
            inw_v[rows, cols] = (w_in * jnp.exp2(end - total)).astype(BF16)
            end_v[b, :, cols] = end
            offcur_v[:, cols] = offcur_v[:, cols] + end

    def state_terms(b):
        rows = pl.ds(b * B, B)
        kept = jnp.exp2(end_v[b])
        for h in range(NH):
            hs = slice(h * DK, (h + 1) * DK)
            st = cur_v[h]
            st_v[b, h] = st
            cur_v[h] = kept[:, hs] * st + dot_tn(v_v[rows, hs], inw_v[rows, hs])

    second[0].wait()
    second[1].wait()
    second[2].wait()
    x_sends[0].wait_recv()
    forget_dots(0)
    value_dots(0)
    for k in range(R // B):
        forget_gate(k)
    for c in range(NT):
        blocks = range(c * R // B, (c + 1) * R // B)
        if c + 1 < NT:
            x_sends[c + 1].wait_recv()
        sums = [forget_sums(b) for b in blocks]
        if c + 1 < NT:
            forget_dots(c + 1)
        else:
            pooled_dots(0)
        for b, part in zip(blocks, sums):
            forget_exps(b, part)
        if c + 1 < NT:
            value_dots(c + 1)
        for b in blocks:
            state_terms(b)
        if c + 1 < NT:
            for b in blocks:
                forget_gate(b + R // B)

    for h in range(NH):
        s1_send[h, pl.ds(0, DK), :] = cur_v[h].astype(BF16)
        s1_send[h, pl.ds(DK, 16), :] = split_rows(offcur_v[0:1, h * DK : (h + 1) * DK])

    def msg1(d):
        to = lax.rem(x + d, NX)
        return send(s1_send.at[to], s1_recv.at[x], m1s_sem.at[d - 1], m1r_sem.at[x], {"sp_1": to})

    def arrival1(d):
        frm = lax.rem(x + d, NX)
        return send(s1_send.at[frm], s1_recv.at[frm], m1s_sem.at[d - 1], m1r_sem.at[frm], {"sp_1": frm})

    for d in (2, 1, 3):
        msg1(d).start()
    for c in w_sends:
        c.start()

    pooled_dots(1)

    halo = send(pooled_v.at[pl.ds(T + B - 16, 16), :], halo_v, hs_sem, hr_sem, next_dev)

    @pl.when(jnp.logical_not(is_last))
    def _():
        halo.start()

    first[3].wait()
    second[3].wait()

    def query_dots(c):
        q = dot(x_v[tile(c), :], wq_v[...])
        up = (silu(q) * explog_v[tile(c), :]).astype(BF16)
        for s in range(R // B):
            rows = pl.ds(c * R + s * B, B)
            for h in range(NH):
                hs = slice(h * DK, (h + 1) * DK)
                u = up[s * B : (s + 1) * B, hs]
                sc = dot_nt(u, down_v[rows, hs])
                sq_v[rows, 2 * h * DK : (2 * h + 1) * DK] = jnp.where(lower, sc, 0.0).astype(BF16)
                sq_v[rows, (2 * h + 1) * DK : (2 * h + 2) * DK] = u

    for c in range(NT):
        query_dots(c)

    def msg2(k):
        return send(s2_send, s2_recv.at[z], m2s_sem.at[k], m2r_sem.at[z], {"sp_0": k})

    def msg3(d):
        to = lax.rem(x + d, NX)
        return send(s3_send.at[to], s3_recv.at[x], m3s_sem.at[d - 1], m3r_sem.at[x], {"sp_1": to})

    def arrival3(d):
        frm = lax.rem(x + d, NX)
        return send(s3_send.at[frm], s3_recv.at[frm], m3s_sem.at[d - 1], m3r_sem.at[frm], {"sp_1": frm})

    def row_prefix():
        s1_recv[x] = s1_send[x]
        for d in range(1, NX):
            arrival1(d).wait_recv()
        run = jnp.zeros((DK, DK), F32)
        logs = jnp.zeros((1, DK), F32)
        for k in range(NX):
            pre_v[k] = run
            bsum_v[k] = jnp.broadcast_to(logs, (8, DK))
            a_k = joined_rows(s1_recv[k, pl.ds(DK, 16), :])
            run = jnp.exp2(a_k) * run + s1_recv[k, pl.ds(0, DK), :].astype(F32)
            logs = logs + a_k
        s2_send[pl.ds(0, DK), :] = run.astype(BF16)
        s2_send[pl.ds(DK, 16), :] = split_rows(logs)

        for k in range(1, nz):

            @pl.when(k > z)
            def _():
                msg2(k).start()

    def column_prefix():
        run_v[...] = jnp.zeros_like(run_v)
        for k in range(nz - 1):

            @pl.when(k < z)
            def _():
                send(s2_send, s2_recv.at[k], m2s_sem.at[k], m2r_sem.at[k], {"sp_0": k}).wait_recv()
                b_k = joined_rows(s2_recv[k, pl.ds(DK, 16), :])
                run_v[...] = jnp.exp2(b_k) * run_v[...] + s2_recv[k, pl.ds(0, DK), :].astype(F32)

        run = run_v[...]
        for k in range(NX):
            s3_send[k] = (jnp.exp2(bsum_v[k][0:1, :]) * run + pre_v[k]).astype(BF16)

        for d in (2, 1, 3):
            msg3(d).start()

    row_at = jnp.where(x == 0, 1, 0)
    column_at = row_at + jnp.where(z == 0, 0, jnp.where(tp == 0, 2, 1))

    def prefixes(at):
        if at <= 1:

            @pl.when(row_at == at)
            def _():
                row_prefix()

        @pl.when(column_at == at)
        def _():
            column_prefix()

    prefixes(0)

    first[4].wait()
    second[4].wait()
    for k in range(2, 7):
        params[k].wait()

    def gate_dots(c):
        g = dot(x_v[tile(c), :], wg_v[...])
        gain = jnp.concatenate([rgain_v[...]] * NH, axis=1)
        gate_v[tile(c), :] = silu(g) * gain

    pool_sends = [
        send(a_v.at[tile(c), pl.ds(0, C)], a_v.at[tile(c), pl.ds(C, C)], ps_sem.at[c], pr_sem.at[c], partner)
        for c in range(NT)
    ]

    def pooling(b):
        position = sp * T + b * B + lax.broadcasted_iota(jnp.int32, (B, 1), 0) + 1
        for g in range(2):
            cols = slice(g * 256, (g + 1) * 256)
            total = dot(band_v[g], pooled_v[pl.ds(b * B, 2 * B), cols])
            here = pooled_v[pl.ds((b + 1) * B, B), cols].astype(F32)
            width = jnp.left_shift(2, 2 * tp + g)
            if b == 0:
                diff = total / jnp.minimum(position, width).astype(F32) - here
            else:
                diff = total * (1.0 / width.astype(F32)) - here
            mixed = dot(diff.astype(BF16), pmix_v[g]) * pscale_v[:, cols]
            a_v[pl.ds(b * B, B), cols] = mixed.astype(BF16)

    def pool_tiles(c):
        for k in range(R // B):
            pooling(c * (R // B) + k)

    gate_dots(0)
    gate_dots(1)
    pool_tiles(1)
    pool_sends[1].start()

    prefixes(1)

    gate_dots(2)
    pool_tiles(2)
    pool_sends[2].start()

    prefixes(2)

    @pl.when(jnp.logical_not(is_first))
    def _():
        halo.wait_recv()
        pooled_v[pl.ds(B - 16, 16), :] = halo_v[...]

    gate_dots(3)
    pool_tiles(3)
    pool_tiles(0)
    pool_sends[3].start()
    pool_sends[0].start()
    prefixes(3)

    for c in out_loads:
        c.wait()
    for c in w_sends:
        c.wait_recv()
    def pool_project(c):
        resid_v[tile(c), :] = ALPHA * x_v[tile(c), 0:H].astype(F32) + dot(
            a_v[tile(c), 0 : 2 * C], wo_v[0 : 2 * C, :]
        )

    for c in range(1, NT):
        pool_sends[c].wait_recv()
        pool_project(c)

    s3_recv[x] = s3_send[x]
    for d in range(1, NX):
        arrival3(d).wait_recv()

    rec_sends = [
        send(
            a_v.at[tile(c), pl.ds(2 * C, C)], a_v.at[tile(c), pl.ds(3 * C, C)],
            rs_sem.at[c], rr_sem.at[c], partner,
        )
        for c in range(NT)
    ]
    stat_sends = [
        send(stat_v.at[tile(c), :], ostat_v.at[tile(c), :], ss_sem.at[c], sr_sem.at[c], partner)
        for c in range(NT)
    ]

    def recur(b):
        rows = pl.ds(b * B, B)
        far = jnp.exp2(off_v[b])
        for h in range(NH):
            hs = slice(h * DK, (h + 1) * DK)
            state = st_v[b, h] + far[:, hs] * s3_recv[h].astype(F32)
            raw = dot(sq_v[rows, 2 * h * DK : (2 * h + 1) * DK], v_v[rows, hs])
            raw = raw + dot_nt(sq_v[rows, (2 * h + 1) * DK : (2 * h + 2) * DK], state.astype(BF16))
            power = jnp.mean(raw * raw, axis=1, keepdims=True)
            normed = raw * lax.rsqrt(power + EPS_RMS) * gate_v[rows, hs]
            a_v[rows, 2 * C + h * DK : 2 * C + (h + 1) * DK] = normed.astype(BF16)

    def project(c):
        resid_v[tile(c), :] = resid_v[tile(c), :] + dot(
            a_v[tile(c), 2 * C : 4 * C], wo_v[2 * C : 4 * C, :]
        )

    def stats(c):
        resid = resid_v[tile(c), :]
        mean = jnp.sum(resid, axis=1, keepdims=True) * (1.0 / H)
        dev = resid - mean
        m2 = jnp.sum(dev * dev, axis=1, keepdims=True)
        lane = lax.broadcasted_iota(jnp.int32, (R, DK), 1)
        stat_v[tile(c), :] = jnp.where(lane == 0, mean, m2)

    def norm(c):
        mine = stat_v[tile(c), :]
        theirs = ostat_v[tile(c), :]
        gap = mine[:, 0:1] - theirs[:, 0:1]
        mean = 0.5 * (mine[:, 0:1] + theirs[:, 0:1])
        var = (mine[:, 1:2] + theirs[:, 1:2] + gap * gap * (0.5 * H)) * (1.0 / (2 * H))
        scale = lax.rsqrt(var + EPS_NORM)
        out[tile(c), :] = (
            (resid_v[tile(c), :] - mean) * scale * ngain_v[...] + nbias_v[...]
        ).astype(BF16)

    def recur_tile(c):
        for k in range(R // B):
            recur(c * (R // B) + k)
        rec_sends[c].start()

    recur_tile(0)
    pool_sends[0].wait_recv()
    for k in range(R // B, 3 * R // B):
        recur(k)
    pool_project(0)
    rec_sends[1].start()
    rec_sends[2].start()
    rec_sends[0].wait_recv()
    for k in range(3 * R // B, T // B):
        recur(k)
    project(0)
    rec_sends[3].start()
    for c in range(1, NT):
        rec_sends[c].wait_recv()
        project(c)
        stats(c - 1)
        stat_sends[c - 1].start()
    stats(NT - 1)
    stat_sends[NT - 1].start()
    for c in range(NT):
        stat_sends[c].wait_recv()
        norm(c)

    for c in range(NT):
        x_sends[c].wait_send()
        pool_sends[c].wait_send()
        rec_sends[c].wait_send()
        stat_sends[c].wait_send()
    for c in w_sends:
        c.wait_send()

    @pl.when(jnp.logical_not(is_last))
    def _():
        halo.wait_send()

    for d in range(1, NX):
        msg1(d).wait_send()
        msg3(d).wait_send()
    for k in range(1, nz):

        @pl.when(k > z)
        def _():
            msg2(k).wait_send()


def layer(nz, *args):
    (stream, wp, wq, wf, wv, wg, pmix, pscale, lb, ed, rgain, wop, wor, ngain, nbias) = args
    sem = pltpu.SemaphoreType.DMA
    scratch = [
        pltpu.VMEM((T, 2 * H), BF16),
        *[pltpu.VMEM((2 * H, C), BF16)] * 5,
        pltpu.VMEM((4 * C, H), BF16),
        pltpu.VMEM((2, 256, 256), BF16),
        pltpu.VMEM((1, C), F32),
        pltpu.VMEM((1, C), F32),
        pltpu.VMEM((NH, T), F32),
        pltpu.VMEM((T, NH), F32),
        pltpu.VMEM((1, DK), F32),
        pltpu.VMEM((1, H), F32),
        pltpu.VMEM((1, H), F32),
        pltpu.VMEM((T, C), F32),
        pltpu.VMEM((4, 2 * B, C), BF16),
        pltpu.VMEM((T, C), BF16),
        pltpu.VMEM((NB, 1, C), F32),
        pltpu.VMEM((T, C), BF16),
        pltpu.VMEM((T, C), F32),
        pltpu.VMEM((T, C), BF16),
        pltpu.VMEM((T + B, C), BF16),
        pltpu.VMEM((16, C), BF16),
        pltpu.VMEM((T, 2 * C), BF16),
        pltpu.VMEM((T, C), F32),
        pltpu.VMEM((T, 4 * C), BF16),
        pltpu.VMEM((NB, NH, DK, DK), F32),
        pltpu.VMEM((NH, DK, DK), F32),
        pltpu.VMEM((NB, 1, C), F32),
        pltpu.VMEM((1, C), F32),
        pltpu.VMEM((2, B, 2 * B), BF16),
        pltpu.VMEM((B, 2 * B), BF16),
        pltpu.VMEM((NH, MSG, DK), BF16),
        pltpu.VMEM((NX, MSG, DK), BF16),
        pltpu.VMEM((MSG, DK), BF16),
        pltpu.VMEM((nz, MSG, DK), BF16),
        pltpu.VMEM((NX, DK, DK), BF16),
        pltpu.VMEM((NX, DK, DK), BF16),
        pltpu.VMEM((NX, DK, DK), F32),
        pltpu.VMEM((NX, 8, DK), F32),
        pltpu.VMEM((DK, DK), F32),
        pltpu.VMEM((T, H), F32),
        pltpu.VMEM((T, DK), F32),
        pltpu.VMEM((T, DK), F32),
        sem((NT + 12,)), sem((7,)),
        sem((NT,)), sem((NT,)), sem((2,)), sem((2,)), sem((NT,)), sem((NT,)),
        sem((NT,)), sem((NT,)), sem((NT,)), sem((NT,)),
        sem, sem,
        sem((NX - 1,)), sem((NX,)), sem((nz,)), sem((nz,)), sem((NX - 1,)), sem((NX,)),
    ]
    operands = (
        stream[0], wp, wq, wf, wv, wg, pmix,
        pscale.reshape(1, C), lb.reshape(1, C), ed.T, rgain.reshape(1, DK),
        wop, wor, ngain.reshape(1, H), nbias.reshape(1, H),
    )
    result = pl.pallas_call(
        functools.partial(kernel, nz),
        out_shape=pltpu.VMEM((T, H), BF16),
        in_specs=[pl.BlockSpec(memory_space=pltpu.HBM)] * 15,
        out_specs=pl.BlockSpec(memory_space=pltpu.VMEM),
        scratch_shapes=scratch,
        compiler_params=pltpu.CompilerParams(
            collective_id=0, has_side_effects=True, vmem_limit_bytes=58_000_000
        ),
    )(*[pltpu.with_memory_space_constraint(a, pltpu.HBM) for a in operands])
    return result[None]


def solution(mesh):
    devices = mesh.devices
    nz = devices.shape[0] // NX
    torus = Mesh(
        devices.reshape(nz, NX, mesh.shape["fs"], mesh.shape["tp"]), ("sp_0", "sp_1", "fs", "tp")
    )
    sp = ("sp_0", "sp_1")
    cols = P(None, "tp")
    return jax.shard_map(
        functools.partial(layer, nz),
        mesh=torus,
        in_specs=(
            P("fs", sp, "tp"), cols, cols, cols, cols, cols,
            P("tp", None, None), P("tp"), P("tp"), P(sp, "tp"), P(),
            P("tp", None), P("tp", None), P("tp"), P("tp"),
        ),
        out_specs=P("fs", sp, "tp"),
        check_vma=False,
    )
```

```python
import functools
import math

import jax
import jax.numpy as jnp
from jax import lax
from jax.experimental import pallas as pl
from jax.experimental.pallas import tpu as pltpu
from jax.sharding import Mesh
from jax.sharding import PartitionSpec as P

BF16 = jnp.bfloat16
F32 = jnp.float32
MESH = pl.DeviceIdType.MESH

ALPHA = 2.0**0.25
EPS_RMS = 1e-06
EPS_NORM = 1e-05
LOG2E = math.log2(math.e)

T = 1024
H = 1024
C = 512
DK = 128
NH = C // DK
B = 128
NB = T // B
R = 256
NT = T // R
RB = 512
NB_BIG = T // RB
NX = 4
MSG = DK + 16


def dot(a, b):
    return jnp.dot(a, b, preferred_element_type=F32)


def dot_tn(a, b):
    return lax.dot_general(a, b, (((0,), (0,)), ((), ())), preferred_element_type=F32)


def dot_nt(a, b):
    return lax.dot_general(a, b, (((1,), (1,)), ((), ())), preferred_element_type=F32)


def silu(x):
    half = 0.5 * x
    return half + half * jnp.tanh(half)


def split_rows(row):
    hi = row.astype(BF16)
    rest = row - hi.astype(F32)
    mid = rest.astype(BF16)
    low = (rest - mid.astype(F32)).astype(BF16)
    rows = lax.broadcasted_iota(jnp.int32, (16, DK), 0)
    return jnp.where(
        rows == 0,
        hi.astype(F32),
        jnp.where(rows == 1, mid.astype(F32), jnp.where(rows == 2, low.astype(F32), 0.0)),
    ).astype(BF16)


def joined_rows(block):
    return jnp.sum(block.astype(F32), axis=0, keepdims=True)


def kernel(
    nz,
    stream, wp, wq, wf, wv, wg, pmix, pscale, lbound, edecay, rgain, wop, wor, ngain, nbias,
    out,
    x_v, wf_v, wv_v, wp_v, wq_v, wg_v, wo_v,
    pmix_v, pscale_v, lb_v, ed_v, edc_v, rgain_v, ngain_v, nbias_v,
    f_v, hl_v, inw_v, end_v, v_v, explog_v, down_v, pooled_v, halo_v, sq_v, gate_v, a_v,
    st_v, cur_v, off_v, offcur_v, band_v, tri_v,
    s1_send, s1_recv, s2_send, s2_recv, s3_send, s3_recv, pre_v, bsum_v, run_v,
    resid_v, stat_v, ostat_v,
    load_sem, param_sem,
    xs_sem, xr_sem, ws_sem, wr_sem, ps_sem, pr_sem, rs_sem, rr_sem, ss_sem, sr_sem,
    hs_sem, hr_sem, m1s_sem, m1r_sem, m2s_sem, m2r_sem, m3s_sem, m3r_sem,
):
    z = lax.axis_index("sp_0")
    x = lax.axis_index("sp_1")
    tp = lax.axis_index("tp")
    sp = z * NX + x
    other = 1 - tp
    n_sp = nz * NX
    after = lax.rem(sp + 1, n_sp)
    prior = lax.rem(sp + n_sp - 1, n_sp)
    is_first, is_last = sp == 0, sp == n_sp - 1
    partner = {"tp": other}
    x_peers = [{"sp_1": lax.rem(x + d, NX)} for d in range(1, NX)]
    z_peers = [{"sp_0": lax.rem(z + d, nz)} for d in range(1, nz)]
    next_dev = {"sp_0": after // NX, "sp_1": lax.rem(after, NX)}
    prev_dev = {"sp_0": prior // NX, "sp_1": lax.rem(prior, NX)}

    barrier = pltpu.get_barrier_semaphore()
    greeted = [partner] + x_peers + z_peers
    for dev in greeted:
        pl.semaphore_signal(barrier, inc=1, device_id=dev, device_id_type=MESH)

    @pl.when(jnp.logical_not(is_last))
    def _():
        pl.semaphore_signal(barrier, inc=1, device_id=next_dev, device_id_type=MESH)

    @pl.when(jnp.logical_not(is_first))
    def _():
        pl.semaphore_signal(barrier, inc=1, device_id=prev_dev, device_id_type=MESH)


    own_half = pl.ds(pl.multiple_of(tp * H, H), H)
    oth_half = pl.ds(pl.multiple_of(other * H, H), H)

    def tile(c):
        return pl.ds(c * R, R)

    def big(c):
        return pl.ds(c * RB, RB)

    loads = [
        pltpu.make_async_copy(stream.at[tile(c), :], x_v.at[tile(c), pl.ds(0, H)], load_sem.at[c])
        for c in range(NT)
    ]
    first, second = {}, {}
    for k, (src, dst) in enumerate(((wf, wf_v), (wv, wv_v), (wp, wp_v), (wq, wq_v), (wg, wg_v))):
        first[k] = pltpu.make_async_copy(
            src.at[own_half, :], dst.at[pl.ds(0, H), :], load_sem.at[NT + 2 * k]
        )
        second[k] = pltpu.make_async_copy(
            src.at[oth_half, :], dst.at[pl.ds(H, H), :], load_sem.at[NT + 2 * k + 1]
        )
    params = [
        pltpu.make_async_copy(src, dst, param_sem.at[k])
        for k, (src, dst) in enumerate(
            (
                (lbound, lb_v), (edecay, ed_v), (pmix, pmix_v), (pscale, pscale_v),
                (rgain, rgain_v), (ngain, ngain_v), (nbias, nbias_v),
            )
        )
    ]
    out_loads = [
        pltpu.make_async_copy(
            src.at[:, own_half], wo_v.at[pl.ds(2 * k * C, C), :], load_sem.at[NT + 10 + k]
        )
        for k, src in enumerate((wop, wor))
    ]
    def start_x(c):
        for k in range(2):
            rows = pl.ds(c * R + k * (R // 2), R // 2)
            pltpu.make_async_copy(stream.at[rows, :], x_v.at[rows, pl.ds(0, H)], load_sem.at[c]).start()

    start_x(0)
    for k in range(4):
        pltpu.make_async_copy(
            wf.at[pl.ds(pl.multiple_of(tp * H + k * 256, 256), 256), :],
            wf_v.at[pl.ds(k * 256, 256), :],
            load_sem.at[NT],
        ).start()
    for c in range(1, NT):
        start_x(c)

    row = lax.broadcasted_iota(jnp.int32, (B, B), 0)
    col = lax.broadcasted_iota(jnp.int32, (B, B), 1)
    lower = row >= col
    ones = jnp.where(lower, 1.0, 0.0).astype(BF16)
    tri_v[:, 0:B] = ones
    tri_v[:, B : 2 * B] = ones
    brow = lax.broadcasted_iota(jnp.int32, (B, 2 * B), 0)
    lag = brow + B - lax.broadcasted_iota(jnp.int32, (B, 2 * B), 1)
    for g in range(2):
        width = jnp.left_shift(2, 2 * tp + g)
        band_v[g] = jnp.where((lag >= 0) & (lag < width), 1.0, 0.0).astype(BF16)
    cur_v[...] = jnp.zeros_like(cur_v)
    offcur_v[...] = jnp.zeros_like(offcur_v)
    pooled_v[pl.ds(0, B), :] = jnp.zeros((B, C), BF16)

    first[0].wait()
    first[1].start()
    for k in range(7):
        params[k].start()
    for c in range(NT):
        loads[c].wait()
        f_v[tile(c), :] = dot(x_v[tile(c), 0:H], wf_v[0:H, :])

    def send(src, dst, s_sem, r_sem, dev):
        return pltpu.make_async_remote_copy(
            src_ref=src, dst_ref=dst, send_sem=s_sem, recv_sem=r_sem, device_id=dev, device_id_type=MESH
        )

    x_sends = [
        send(
            x_v.at[tile(c), pl.ds(0, H)], x_v.at[tile(c), pl.ds(H, H)],
            xs_sem.at[c], xr_sem.at[c], partner,
        )
        for c in range(NT)
    ]
    def meet_and_send():
        pl.semaphore_wait(barrier, len(greeted) + jnp.minimum(sp, 1) + jnp.minimum(n_sp - 1 - sp, 1))
        for c in x_sends:
            c.start()

    @pl.when(z > 0)
    def _():
        meet_and_send()

    first[2].start()
    for k in (0, 1, 2):
        second[k].start()

    first[1].wait()
    for c in range(NB_BIG):
        resid_v[big(c), 0:C] = dot(x_v[big(c), 0:H], wv_v[0:H, :])
    @pl.when(z == 0)
    def _():
        meet_and_send()

    w_sends = [
        send(
            src.at[:, oth_half], wo_v.at[pl.ds((2 * k + 1) * C, C), :], ws_sem.at[k], wr_sem.at[k], partner
        )
        for k, src in enumerate((wop, wor))
    ]

    first[2].wait()
    resid_v[big(0), C : 2 * C] = dot(x_v[big(0), 0:H], wp_v[0:H, :])

    @pl.when(z == 0)
    def _():
        resid_v[big(1), C : 2 * C] = dot(x_v[big(1), 0:H], wp_v[0:H, :])

    for k in (3, 4):
        first[k].start()
        second[k].start()
    for c in out_loads:
        c.start()
    params[0].wait()
    params[1].wait()
    for b in range(NB):
        edc_v[pl.ds(b * B, B), :] = jnp.transpose(ed_v[:, b * B : (b + 1) * B] * LOG2E)

    def forget_dots(c):
        f_v[tile(c), :] = f_v[tile(c), :] + dot(x_v[tile(c), H : 2 * H], wf_v[H : 2 * H, :])

    def value_dots(c):
        v_v[tile(c), :] = (
            resid_v[tile(c), 0:C] + dot(x_v[tile(c), H : 2 * H], wv_v[H : 2 * H, :])
        ).astype(BF16)

    def pooled_rest(c):
        pooled_v[pl.ds(c * RB + B, RB), :] = (
            resid_v[big(c), C : 2 * C] + dot(x_v[big(c), H : 2 * H], wp_v[H : 2 * H, :])
        ).astype(BF16)

    def pooled_whole(c):
        pooled_v[pl.ds(c * RB + B, RB), :] = dot(x_v[big(c), :], wp_v[...]).astype(BF16)

    def forget_gate(b):
        rows = pl.ds(b * B, B)
        ed = edc_v[rows, :]
        for h in range(NH):
            cols = slice(h * DK, (h + 1) * DK)
            half_gap = 0.5 - 0.5 * lb_v[:, cols]
            w_in = half_gap - half_gap * jnp.tanh(0.5 * f_v[rows, cols])
            f_v[rows, cols] = w_in
            keep = jnp.log(1.0 - w_in) * LOG2E + ed[:, h : h + 1]
            hi = keep.astype(BF16)
            hl_v[b % 4, 0:B, cols] = hi
            hl_v[b % 4, B : 2 * B, cols] = (keep - hi.astype(F32)).astype(BF16)

    def forget_sums(b):
        return [dot(tri_v[...], hl_v[b % 4, :, 2 * p * DK : 2 * (p + 1) * DK]) for p in range(NH // 2)]

    def forget_exps(b, sums):
        rows = pl.ds(b * B, B)
        off_v[b] = offcur_v[...]
        for p in range(NH // 2):
            cols = slice(2 * p * DK, 2 * (p + 1) * DK)
            total = sums[p]
            end = total[B - 1 : B, :]
            w_in = f_v[rows, cols]
            explog_v[rows, cols] = jnp.exp2(total)
            down_v[rows, cols] = (w_in * jnp.exp2(-total)).astype(BF16)
            inw_v[rows, cols] = (w_in * jnp.exp2(end - total)).astype(BF16)
            end_v[b, :, cols] = end
            offcur_v[:, cols] = offcur_v[:, cols] + end

    def state_terms(b):
        rows = pl.ds(b * B, B)
        kept = jnp.exp2(end_v[b])
        for h in range(NH):
            hs = slice(h * DK, (h + 1) * DK)
            st = cur_v[h]
            st_v[b, h] = st
            cur_v[h] = kept[:, hs] * st + dot_tn(v_v[rows, hs], inw_v[rows, hs])

    second[0].wait()
    second[1].wait()
    second[2].wait()
    x_sends[0].wait_recv()
    forget_dots(0)
    value_dots(0)
    for k in range(R // B):
        forget_gate(k)
    for c in range(NT):
        blocks = range(c * R // B, (c + 1) * R // B)
        if c + 1 < NT:
            x_sends[c + 1].wait_recv()
        sums = [forget_sums(b) for b in blocks]
        if c + 1 < NT:
            forget_dots(c + 1)
        for b, part in zip(blocks, sums):
            forget_exps(b, part)
        if c + 1 < NT:
            value_dots(c + 1)
        for b in blocks:
            state_terms(b)
        if c + 1 < NT:
            for b in blocks:
                forget_gate(b + R // B)

    for h in range(NH):
        s1_send[h, pl.ds(0, DK), :] = cur_v[h].astype(BF16)
        s1_send[h, pl.ds(DK, 16), :] = split_rows(offcur_v[0:1, h * DK : (h + 1) * DK])

    def msg1(d):
        to = lax.rem(x + d, NX)
        return send(s1_send.at[to], s1_recv.at[x], m1s_sem.at[d - 1], m1r_sem.at[x], {"sp_1": to})

    def arrival1(d):
        frm = lax.rem(x + d, NX)
        return send(s1_send.at[frm], s1_recv.at[frm], m1s_sem.at[d - 1], m1r_sem.at[frm], {"sp_1": frm})

    for d in (2, 1, 3):
        msg1(d).start()
    for c in w_sends:
        c.start()

    pooled_rest(0)

    @pl.when(z == 0)
    def _():
        pooled_rest(1)

    @pl.when(z > 0)
    def _():
        pooled_whole(1)


    halo = send(pooled_v.at[pl.ds(T + B - 16, 16), :], halo_v, hs_sem, hr_sem, next_dev)

    @pl.when(jnp.logical_not(is_last))
    def _():
        halo.start()

    first[3].wait()
    second[3].wait()

    def query_dots(c):
        q = dot(x_v[tile(c), :], wq_v[...])
        up = (silu(q) * explog_v[tile(c), :]).astype(BF16)
        for s in range(R // B):
            rows = pl.ds(c * R + s * B, B)
            for h in range(NH):
                hs = slice(h * DK, (h + 1) * DK)
                u = up[s * B : (s + 1) * B, hs]
                sc = dot_nt(u, down_v[rows, hs])
                sq_v[rows, 2 * h * DK : (2 * h + 1) * DK] = jnp.where(lower, sc, 0.0).astype(BF16)
                sq_v[rows, (2 * h + 1) * DK : (2 * h + 2) * DK] = u

    def msg2(k):
        return send(s2_send, s2_recv.at[z], m2s_sem.at[k], m2r_sem.at[z], {"sp_0": k})

    def msg3(d):
        to = lax.rem(x + d, NX)
        return send(s3_send.at[to], s3_recv.at[x], m3s_sem.at[d - 1], m3r_sem.at[x], {"sp_1": to})

    def arrival3(d):
        frm = lax.rem(x + d, NX)
        return send(s3_send.at[frm], s3_recv.at[frm], m3s_sem.at[d - 1], m3r_sem.at[frm], {"sp_1": frm})

    def row_prefix():
        s1_recv[x] = s1_send[x]
        for d in range(1, NX):
            arrival1(d).wait_recv()
        run = jnp.zeros((DK, DK), F32)
        logs = jnp.zeros((1, DK), F32)
        for k in range(NX):
            pre_v[k] = run
            bsum_v[k] = jnp.broadcast_to(logs, (8, DK))
            a_k = joined_rows(s1_recv[k, pl.ds(DK, 16), :])
            run = jnp.exp2(a_k) * run + s1_recv[k, pl.ds(0, DK), :].astype(F32)
            logs = logs + a_k
        s2_send[pl.ds(0, DK), :] = run.astype(BF16)
        s2_send[pl.ds(DK, 16), :] = split_rows(logs)

        for k in range(1, nz):

            @pl.when(k > z)
            def _():
                msg2(k).start()

    def column_prefix():
        run_v[...] = jnp.zeros_like(run_v)
        for k in range(nz - 1):

            @pl.when(k < z)
            def _():
                send(s2_send, s2_recv.at[k], m2s_sem.at[k], m2r_sem.at[k], {"sp_0": k}).wait_recv()
                b_k = joined_rows(s2_recv[k, pl.ds(DK, 16), :])
                run_v[...] = jnp.exp2(b_k) * run_v[...] + s2_recv[k, pl.ds(0, DK), :].astype(F32)

        run = run_v[...]
        for k in range(NX):
            s3_send[k] = (jnp.exp2(bsum_v[k][0:1, :]) * run + pre_v[k]).astype(BF16)

        for d in (2, 1, 3):
            msg3(d).start()

    row_at = jnp.where(x == 0, 1, 0)
    column_at = jnp.where(z == 0, row_at, 2 + row_at)

    def prefixes(at):
        if at <= 1:

            @pl.when(row_at == at)
            def _():
                row_prefix()

        @pl.when(column_at == at)
        def _():
            column_prefix()

    for c in range(NT - 1):
        query_dots(c)
    prefixes(0)
    query_dots(NT - 1)
    prefixes(1)

    first[4].wait()
    second[4].wait()
    for k in range(2, 7):
        params[k].wait()

    def gate_dots(c):
        g = dot(x_v[tile(c), :], wg_v[...])
        gain = jnp.concatenate([rgain_v[...]] * NH, axis=1)
        gate_v[tile(c), :] = silu(g) * gain

    pool_sends = [
        send(a_v.at[tile(c), pl.ds(0, C)], a_v.at[tile(c), pl.ds(C, C)], ps_sem.at[c], pr_sem.at[c], partner)
        for c in range(NT)
    ]

    def pooling(b):
        position = sp * T + b * B + lax.broadcasted_iota(jnp.int32, (B, 1), 0) + 1
        for g in range(2):
            cols = slice(g * 256, (g + 1) * 256)
            total = dot(band_v[g], pooled_v[pl.ds(b * B, 2 * B), cols])
            here = pooled_v[pl.ds((b + 1) * B, B), cols].astype(F32)
            width = jnp.left_shift(2, 2 * tp + g)
            if b == 0:
                diff = total / jnp.minimum(position, width).astype(F32) - here
            else:
                diff = total * (1.0 / width.astype(F32)) - here
            mixed = dot(diff.astype(BF16), pmix_v[g]) * pscale_v[:, cols]
            a_v[pl.ds(b * B, B), cols] = mixed.astype(BF16)

    def pool_tiles(c):
        for k in range(R // B):
            pooling(c * (R // B) + k)

    gate_dots(0)
    gate_dots(1)
    pool_tiles(1)
    pool_sends[1].start()

    prefixes(2)

    gate_dots(2)
    gate_dots(3)
    pool_tiles(2)
    pool_sends[2].start()
    prefixes(3)

    @pl.when(jnp.logical_not(is_first))
    def _():
        halo.wait_recv()
        pooled_v[pl.ds(B - 16, 16), :] = halo_v[...]

    pool_tiles(3)
    pool_tiles(0)
    pool_sends[3].start()
    pool_sends[0].start()

    for c in out_loads:
        c.wait()
    for c in w_sends:
        c.wait_recv()
    def pool_project(c):
        resid_v[tile(c), :] = ALPHA * x_v[tile(c), 0:H].astype(F32) + dot(
            a_v[tile(c), 0 : 2 * C], wo_v[0 : 2 * C, :]
        )

    for c in range(1, NT):
        pool_sends[c].wait_recv()
        pool_project(c)

    s3_recv[x] = s3_send[x]
    for d in range(1, NX):
        arrival3(d).wait_recv()

    rec_sends = [
        send(
            a_v.at[tile(c), pl.ds(2 * C, C)], a_v.at[tile(c), pl.ds(3 * C, C)],
            rs_sem.at[c], rr_sem.at[c], partner,
        )
        for c in range(NT)
    ]
    stat_sends = [
        send(stat_v.at[tile(c), :], ostat_v.at[tile(c), :], ss_sem.at[c], sr_sem.at[c], partner)
        for c in range(NT)
    ]

    def recur(b):
        rows = pl.ds(b * B, B)
        far = jnp.exp2(off_v[b])
        for h in range(NH):
            hs = slice(h * DK, (h + 1) * DK)
            state = st_v[b, h] + far[:, hs] * s3_recv[h].astype(F32)
            raw = dot(sq_v[rows, 2 * h * DK : (2 * h + 1) * DK], v_v[rows, hs])
            raw = raw + dot_nt(sq_v[rows, (2 * h + 1) * DK : (2 * h + 2) * DK], state.astype(BF16))
            power = jnp.mean(raw * raw, axis=1, keepdims=True)
            normed = raw * lax.rsqrt(power + EPS_RMS) * gate_v[rows, hs]
            a_v[rows, 2 * C + h * DK : 2 * C + (h + 1) * DK] = normed.astype(BF16)

    def project(c):
        resid_v[tile(c), :] = resid_v[tile(c), :] + dot(
            a_v[tile(c), 2 * C : 4 * C], wo_v[2 * C : 4 * C, :]
        )

    def stats(c):
        resid = resid_v[tile(c), :]
        mean = jnp.sum(resid, axis=1, keepdims=True) * (1.0 / H)
        dev = resid - mean
        m2 = jnp.sum(dev * dev, axis=1, keepdims=True)
        lane = lax.broadcasted_iota(jnp.int32, (R, DK), 1)
        stat_v[tile(c), :] = jnp.where(lane == 0, mean, m2)

    def norm(c):
        mine = stat_v[tile(c), :]
        theirs = ostat_v[tile(c), :]
        gap = mine[:, 0:1] - theirs[:, 0:1]
        mean = 0.5 * (mine[:, 0:1] + theirs[:, 0:1])
        var = (mine[:, 1:2] + theirs[:, 1:2] + gap * gap * (0.5 * H)) * (1.0 / (2 * H))
        scale = lax.rsqrt(var + EPS_NORM)
        out[tile(c), :] = (
            (resid_v[tile(c), :] - mean) * scale * ngain_v[...] + nbias_v[...]
        ).astype(BF16)

    def recur_tile(c):
        for k in range(R // B):
            recur(c * (R // B) + k)
        rec_sends[c].start()

    recur_tile(0)
    pool_sends[0].wait_recv()
    for k in range(R // B, 3 * R // B):
        recur(k)
    pool_project(0)
    rec_sends[1].start()
    rec_sends[2].start()
    rec_sends[0].wait_recv()
    for k in range(3 * R // B, T // B):
        recur(k)
    project(0)
    rec_sends[3].start()
    for c in range(1, NT):
        rec_sends[c].wait_recv()
        project(c)
        stats(c - 1)
        stat_sends[c - 1].start()
    stats(NT - 1)
    stat_sends[NT - 1].start()
    for group in ((0, 1), (2,), (3,)):
        for c in group:
            stat_sends[c].wait_recv()
        for c in group:
            norm(c)

    for c in range(NT):
        x_sends[c].wait_send()
        pool_sends[c].wait_send()
        rec_sends[c].wait_send()
        stat_sends[c].wait_send()
    for c in w_sends:
        c.wait_send()

    @pl.when(jnp.logical_not(is_last))
    def _():
        halo.wait_send()

    for d in range(1, NX):
        msg1(d).wait_send()
        msg3(d).wait_send()
    for k in range(1, nz):

        @pl.when(k > z)
        def _():
            msg2(k).wait_send()


def layer(nz, *args):
    (stream, wp, wq, wf, wv, wg, pmix, pscale, lb, ed, rgain, wop, wor, ngain, nbias) = args
    sem = pltpu.SemaphoreType.DMA
    scratch = [
        pltpu.VMEM((T, 2 * H), BF16),
        *[pltpu.VMEM((2 * H, C), BF16)] * 5,
        pltpu.VMEM((4 * C, H), BF16),
        pltpu.VMEM((2, 256, 256), BF16),
        pltpu.VMEM((1, C), F32),
        pltpu.VMEM((1, C), F32),
        pltpu.VMEM((NH, T), F32),
        pltpu.VMEM((T, NH), F32),
        pltpu.VMEM((1, DK), F32),
        pltpu.VMEM((1, H), F32),
        pltpu.VMEM((1, H), F32),
        pltpu.VMEM((T, C), F32),
        pltpu.VMEM((4, 2 * B, C), BF16),
        pltpu.VMEM((T, C), BF16),
        pltpu.VMEM((NB, 1, C), F32),
        pltpu.VMEM((T, C), BF16),
        pltpu.VMEM((T, C), F32),
        pltpu.VMEM((T, C), BF16),
        pltpu.VMEM((T + B, C), BF16),
        pltpu.VMEM((16, C), BF16),
        pltpu.VMEM((T, 2 * C), BF16),
        pltpu.VMEM((T, C), F32),
        pltpu.VMEM((T, 4 * C), BF16),
        pltpu.VMEM((NB, NH, DK, DK), F32),
        pltpu.VMEM((NH, DK, DK), F32),
        pltpu.VMEM((NB, 1, C), F32),
        pltpu.VMEM((1, C), F32),
        pltpu.VMEM((2, B, 2 * B), BF16),
        pltpu.VMEM((B, 2 * B), BF16),
        pltpu.VMEM((NH, MSG, DK), BF16),
        pltpu.VMEM((NX, MSG, DK), BF16),
        pltpu.VMEM((MSG, DK), BF16),
        pltpu.VMEM((nz, MSG, DK), BF16),
        pltpu.VMEM((NX, DK, DK), BF16),
        pltpu.VMEM((NX, DK, DK), BF16),
        pltpu.VMEM((NX, DK, DK), F32),
        pltpu.VMEM((NX, 8, DK), F32),
        pltpu.VMEM((DK, DK), F32),
        pltpu.VMEM((T, H), F32),
        pltpu.VMEM((T, DK), F32),
        pltpu.VMEM((T, DK), F32),
        sem((NT + 12,)), sem((7,)),
        sem((NT,)), sem((NT,)), sem((2,)), sem((2,)), sem((NT,)), sem((NT,)),
        sem((NT,)), sem((NT,)), sem((NT,)), sem((NT,)),
        sem, sem,
        sem((NX - 1,)), sem((NX,)), sem((nz,)), sem((nz,)), sem((NX - 1,)), sem((NX,)),
    ]
    operands = (
        stream[0], wp, wq, wf, wv, wg, pmix,
        pscale.reshape(1, C), lb.reshape(1, C), ed.T, rgain.reshape(1, DK),
        wop, wor, ngain.reshape(1, H), nbias.reshape(1, H),
    )
    result = pl.pallas_call(
        functools.partial(kernel, nz),
        out_shape=pltpu.VMEM((T, H), BF16),
        in_specs=[pl.BlockSpec(memory_space=pltpu.HBM)] * 15,
        out_specs=pl.BlockSpec(memory_space=pltpu.VMEM),
        scratch_shapes=scratch,
        compiler_params=pltpu.CompilerParams(
            collective_id=0, has_side_effects=True, vmem_limit_bytes=58_000_000
        ),
    )(*[pltpu.with_memory_space_constraint(a, pltpu.HBM) for a in operands])
    return result[None]


def solution(mesh):
    devices = mesh.devices
    nz = devices.shape[0] // NX
    torus = Mesh(
        devices.reshape(nz, NX, mesh.shape["fs"], mesh.shape["tp"]), ("sp_0", "sp_1", "fs", "tp")
    )
    sp = ("sp_0", "sp_1")
    cols = P(None, "tp")
    return jax.shard_map(
        functools.partial(layer, nz),
        mesh=torus,
        in_specs=(
            P("fs", sp, "tp"), cols, cols, cols, cols, cols,
            P("tp", None, None), P("tp"), P("tp"), P(sp, "tp"), P(),
            P("tp", None), P("tp", None), P("tp"), P("tp"),
        ),
        out_specs=P("fs", sp, "tp"),
        check_vma=False,
    )
```

```python
import functools
import math

import jax
import jax.numpy as jnp
from jax import lax
from jax.experimental import pallas as pl
from jax.experimental.pallas import tpu as pltpu
from jax.sharding import Mesh
from jax.sharding import PartitionSpec as P

BF16 = jnp.bfloat16
F32 = jnp.float32
MESH = pl.DeviceIdType.MESH

ALPHA = 2.0**0.25
EPS_RMS = 1e-06
EPS_NORM = 1e-05
LOG2E = math.log2(math.e)

T = 1024
H = 1024
C = 512
DK = 128
NH = C // DK
B = 128
NB = T // B
R = 256
NT = T // R
RB = 512
NB_BIG = T // RB
NX = 4
MSG = DK + 16


def dot(a, b):
    return jnp.dot(a, b, preferred_element_type=F32)


def dot_tn(a, b):
    return lax.dot_general(a, b, (((0,), (0,)), ((), ())), preferred_element_type=F32)


def dot_nt(a, b):
    return lax.dot_general(a, b, (((1,), (1,)), ((), ())), preferred_element_type=F32)


def silu(x):
    half = 0.5 * x
    return half + half * jnp.tanh(half)


def split_rows(row):
    hi = row.astype(BF16)
    rest = row - hi.astype(F32)
    mid = rest.astype(BF16)
    low = (rest - mid.astype(F32)).astype(BF16)
    rows = lax.broadcasted_iota(jnp.int32, (16, DK), 0)
    return jnp.where(
        rows == 0,
        hi.astype(F32),
        jnp.where(rows == 1, mid.astype(F32), jnp.where(rows == 2, low.astype(F32), 0.0)),
    ).astype(BF16)


def joined_rows(block):
    return jnp.sum(block.astype(F32), axis=0, keepdims=True)


def kernel(
    nz,
    stream, wp, wq, wf, wv, wg, pmix, pscale, lbound, edecay, rgain, wop, wor, ngain, nbias,
    out,
    x_v, wf_v, wv_v, wp_v, wq_v, wg_v, wo_v,
    pmix_v, pscale_v, lb_v, ed_v, edc_v, rgain_v, ngain_v, nbias_v,
    f_v, hl_v, inw_v, end_v, v_v, explog_v, down_v, pooled_v, halo_v, sq_v, gate_v, a_v,
    st_v, cur_v, off_v, offcur_v, band_v, tri_v,
    s1_send, s1_recv, s2_send, s2_recv, s3_send, s3_recv, pre_v, bsum_v, run_v,
    resid_v, stat_v, ostat_v,
    load_sem, param_sem,
    xs_sem, xr_sem, ws_sem, wr_sem, ps_sem, pr_sem, rs_sem, rr_sem, ss_sem, sr_sem,
    hs_sem, hr_sem, m1s_sem, m1r_sem, m2s_sem, m2r_sem, m3s_sem, m3r_sem,
):
    z = lax.axis_index("sp_0")
    x = lax.axis_index("sp_1")
    tp = lax.axis_index("tp")
    sp = z * NX + x
    other = 1 - tp
    n_sp = nz * NX
    after = lax.rem(sp + 1, n_sp)
    prior = lax.rem(sp + n_sp - 1, n_sp)
    is_first, is_last = sp == 0, sp == n_sp - 1
    partner = {"tp": other}
    x_peers = [{"sp_1": lax.rem(x + d, NX)} for d in range(1, NX)]
    z_peers = [{"sp_0": lax.rem(z + d, nz)} for d in range(1, nz)]
    next_dev = {"sp_0": after // NX, "sp_1": lax.rem(after, NX)}
    prev_dev = {"sp_0": prior // NX, "sp_1": lax.rem(prior, NX)}

    barrier = pltpu.get_barrier_semaphore()
    greeted = [partner] + x_peers + z_peers
    for dev in greeted:
        pl.semaphore_signal(barrier, inc=1, device_id=dev, device_id_type=MESH)

    @pl.when(jnp.logical_not(is_last))
    def _():
        pl.semaphore_signal(barrier, inc=1, device_id=next_dev, device_id_type=MESH)

    @pl.when(jnp.logical_not(is_first))
    def _():
        pl.semaphore_signal(barrier, inc=1, device_id=prev_dev, device_id_type=MESH)


    own_half = pl.ds(pl.multiple_of(tp * H, H), H)
    oth_half = pl.ds(pl.multiple_of(other * H, H), H)

    def tile(c):
        return pl.ds(c * R, R)

    def big(c):
        return pl.ds(c * RB, RB)

    loads = [
        pltpu.make_async_copy(stream.at[tile(c), :], x_v.at[tile(c), pl.ds(0, H)], load_sem.at[c])
        for c in range(NT)
    ]
    first, second = {}, {}
    for k, (src, dst) in enumerate(((wf, wf_v), (wv, wv_v), (wp, wp_v), (wq, wq_v), (wg, wg_v))):
        first[k] = pltpu.make_async_copy(
            src.at[own_half, :], dst.at[pl.ds(0, H), :], load_sem.at[NT + 2 * k]
        )
        second[k] = pltpu.make_async_copy(
            src.at[oth_half, :], dst.at[pl.ds(H, H), :], load_sem.at[NT + 2 * k + 1]
        )
    params = [
        pltpu.make_async_copy(src, dst, param_sem.at[k])
        for k, (src, dst) in enumerate(
            (
                (lbound, lb_v), (edecay, ed_v), (pmix, pmix_v), (pscale, pscale_v),
                (rgain, rgain_v), (ngain, ngain_v), (nbias, nbias_v),
            )
        )
    ]
    out_loads = [
        pltpu.make_async_copy(
            src.at[:, own_half], wo_v.at[pl.ds(2 * k * C, C), :], load_sem.at[NT + 10 + k]
        )
        for k, src in enumerate((wop, wor))
    ]
    def start_x(c):
        for k in range(2):
            rows = pl.ds(c * R + k * (R // 2), R // 2)
            pltpu.make_async_copy(stream.at[rows, :], x_v.at[rows, pl.ds(0, H)], load_sem.at[c]).start()

    start_x(0)
    for k in range(4):
        pltpu.make_async_copy(
            wf.at[pl.ds(pl.multiple_of(tp * H + k * 256, 256), 256), :],
            wf_v.at[pl.ds(k * 256, 256), :],
            load_sem.at[NT],
        ).start()
    for c in range(1, NT):
        start_x(c)

    row = lax.broadcasted_iota(jnp.int32, (B, B), 0)
    col = lax.broadcasted_iota(jnp.int32, (B, B), 1)
    lower = row >= col
    ones = jnp.where(lower, 1.0, 0.0).astype(BF16)
    tri_v[:, 0:B] = ones
    tri_v[:, B : 2 * B] = ones
    brow = lax.broadcasted_iota(jnp.int32, (B, 2 * B), 0)
    lag = brow + B - lax.broadcasted_iota(jnp.int32, (B, 2 * B), 1)
    for g in range(2):
        width = jnp.left_shift(2, 2 * tp + g)
        band_v[g] = jnp.where((lag >= 0) & (lag < width), 1.0, 0.0).astype(BF16)
    cur_v[...] = jnp.zeros_like(cur_v)
    offcur_v[...] = jnp.zeros_like(offcur_v)
    pooled_v[pl.ds(0, B), :] = jnp.zeros((B, C), BF16)

    first[0].wait()
    first[1].start()
    for k in range(7):
        params[k].start()
    for c in range(NT):
        loads[c].wait()
        f_v[tile(c), :] = dot(x_v[tile(c), 0:H], wf_v[0:H, :])

    first[2].start()
    for k in (0, 1, 2):
        second[k].start()

    first[1].wait()
    for c in range(NB_BIG):
        resid_v[big(c), 0:C] = dot(x_v[big(c), 0:H], wv_v[0:H, :])
    pl.semaphore_wait(barrier, len(greeted) + jnp.minimum(sp, 1) + jnp.minimum(n_sp - 1 - sp, 1))

    def send(src, dst, s_sem, r_sem, dev):
        return pltpu.make_async_remote_copy(
            src_ref=src, dst_ref=dst, send_sem=s_sem, recv_sem=r_sem, device_id=dev, device_id_type=MESH
        )

    x_sends = [
        send(
            x_v.at[tile(c), pl.ds(0, H)], x_v.at[tile(c), pl.ds(H, H)],
            xs_sem.at[c], xr_sem.at[c], partner,
        )
        for c in range(NT)
    ]
    for c in x_sends:
        c.start()
    w_sends = [
        send(
            src.at[:, oth_half], wo_v.at[pl.ds((2 * k + 1) * C, C), :], ws_sem.at[k], wr_sem.at[k], partner
        )
        for k, src in enumerate((wop, wor))
    ]

    first[2].wait()
    for c in range(NB_BIG):
        resid_v[big(c), C : 2 * C] = dot(x_v[big(c), 0:H], wp_v[0:H, :])
    for k in (3, 4):
        first[k].start()
        second[k].start()
    for c in out_loads:
        c.start()
    params[0].wait()
    params[1].wait()
    for b in range(NB):
        edc_v[pl.ds(b * B, B), :] = jnp.transpose(ed_v[:, b * B : (b + 1) * B] * LOG2E)

    def forget_dots(c):
        f_v[tile(c), :] = f_v[tile(c), :] + dot(x_v[tile(c), H : 2 * H], wf_v[H : 2 * H, :])

    def value_dots(c):
        v_v[tile(c), :] = (
            resid_v[tile(c), 0:C] + dot(x_v[tile(c), H : 2 * H], wv_v[H : 2 * H, :])
        ).astype(BF16)

    def pooled_dots(c):
        pooled_v[pl.ds(c * RB + B, RB), :] = (
            resid_v[big(c), C : 2 * C] + dot(x_v[big(c), H : 2 * H], wp_v[H : 2 * H, :])
        ).astype(BF16)

    def forget_gate(b):
        rows = pl.ds(b * B, B)
        ed = edc_v[rows, :]
        for h in range(NH):
            cols = slice(h * DK, (h + 1) * DK)
            half_gap = 0.5 - 0.5 * lb_v[:, cols]
            w_in = half_gap - half_gap * jnp.tanh(0.5 * f_v[rows, cols])
            f_v[rows, cols] = w_in
            keep = jnp.log(1.0 - w_in) * LOG2E + ed[:, h : h + 1]
            hi = keep.astype(BF16)
            hl_v[b % 4, 0:B, cols] = hi
            hl_v[b % 4, B : 2 * B, cols] = (keep - hi.astype(F32)).astype(BF16)

    def forget_sums(b):
        return [dot(tri_v[...], hl_v[b % 4, :, 2 * p * DK : 2 * (p + 1) * DK]) for p in range(NH // 2)]

    def forget_exps(b, sums):
        rows = pl.ds(b * B, B)
        off_v[b] = offcur_v[...]
        for p in range(NH // 2):
            cols = slice(2 * p * DK, 2 * (p + 1) * DK)
            total = sums[p]
            end = total[B - 1 : B, :]
            w_in = f_v[rows, cols]
            explog_v[rows, cols] = jnp.exp2(total)
            down_v[rows, cols] = (w_in * jnp.exp2(-total)).astype(BF16)
            inw_v[rows, cols] = (w_in * jnp.exp2(end - total)).astype(BF16)
            end_v[b, :, cols] = end
            offcur_v[:, cols] = offcur_v[:, cols] + end

    def state_terms(b):
        rows = pl.ds(b * B, B)
        kept = jnp.exp2(end_v[b])
        for h in range(NH):
            hs = slice(h * DK, (h + 1) * DK)
            st = cur_v[h]
            st_v[b, h] = st
            cur_v[h] = kept[:, hs] * st + dot_tn(v_v[rows, hs], inw_v[rows, hs])

    second[0].wait()
    second[1].wait()
    second[2].wait()
    x_sends[0].wait_recv()
    forget_dots(0)
    value_dots(0)
    for k in range(R // B):
        forget_gate(k)
    for c in range(NT):
        blocks = range(c * R // B, (c + 1) * R // B)
        if c + 1 < NT:
            x_sends[c + 1].wait_recv()
        sums = [forget_sums(b) for b in blocks]
        if c + 1 < NT:
            forget_dots(c + 1)
        else:
            pooled_dots(0)
        for b, part in zip(blocks, sums):
            forget_exps(b, part)
        if c + 1 < NT:
            value_dots(c + 1)
        for b in blocks:
            state_terms(b)
        if c + 1 < NT:
            for b in blocks:
                forget_gate(b + R // B)

    for h in range(NH):
        s1_send[h, pl.ds(0, DK), :] = cur_v[h].astype(BF16)
        s1_send[h, pl.ds(DK, 16), :] = split_rows(offcur_v[0:1, h * DK : (h + 1) * DK])

    def msg1(d):
        to = lax.rem(x + d, NX)
        return send(s1_send.at[to], s1_recv.at[x], m1s_sem.at[d - 1], m1r_sem.at[x], {"sp_1": to})

    def arrival1(d):
        frm = lax.rem(x + d, NX)
        return send(s1_send.at[frm], s1_recv.at[frm], m1s_sem.at[d - 1], m1r_sem.at[frm], {"sp_1": frm})

    for d in (2, 1, 3):
        msg1(d).start()
    for c in w_sends:
        c.start()

    pooled_dots(1)

    halo = send(pooled_v.at[pl.ds(T + B - 16, 16), :], halo_v, hs_sem, hr_sem, next_dev)

    @pl.when(jnp.logical_not(is_last))
    def _():
        halo.start()

    first[3].wait()
    second[3].wait()

    def query_dots(c):
        q = dot(x_v[tile(c), :], wq_v[...])
        up = (silu(q) * explog_v[tile(c), :]).astype(BF16)
        for s in range(R // B):
            rows = pl.ds(c * R + s * B, B)
            for h in range(NH):
                hs = slice(h * DK, (h + 1) * DK)
                u = up[s * B : (s + 1) * B, hs]
                sc = dot_nt(u, down_v[rows, hs])
                sq_v[rows, 2 * h * DK : (2 * h + 1) * DK] = jnp.where(lower, sc, 0.0).astype(BF16)
                sq_v[rows, (2 * h + 1) * DK : (2 * h + 2) * DK] = u

    for c in range(NT):
        query_dots(c)

    def msg2(k):
        return send(s2_send, s2_recv.at[z], m2s_sem.at[k], m2r_sem.at[z], {"sp_0": k})

    def msg3(d):
        to = lax.rem(x + d, NX)
        return send(s3_send.at[to], s3_recv.at[x], m3s_sem.at[d - 1], m3r_sem.at[x], {"sp_1": to})

    def arrival3(d):
        frm = lax.rem(x + d, NX)
        return send(s3_send.at[frm], s3_recv.at[frm], m3s_sem.at[d - 1], m3r_sem.at[frm], {"sp_1": frm})

    def row_prefix():
        s1_recv[x] = s1_send[x]
        for d in range(1, NX):
            arrival1(d).wait_recv()
        run = jnp.zeros((DK, DK), F32)
        logs = jnp.zeros((1, DK), F32)
        for k in range(NX):
            pre_v[k] = run
            bsum_v[k] = jnp.broadcast_to(logs, (8, DK))
            a_k = joined_rows(s1_recv[k, pl.ds(DK, 16), :])
            run = jnp.exp2(a_k) * run + s1_recv[k, pl.ds(0, DK), :].astype(F32)
            logs = logs + a_k
        s2_send[pl.ds(0, DK), :] = run.astype(BF16)
        s2_send[pl.ds(DK, 16), :] = split_rows(logs)

        for k in range(1, nz):

            @pl.when(k > z)
            def _():
                msg2(k).start()

    def column_prefix():
        run_v[...] = jnp.zeros_like(run_v)
        for k in range(nz - 1):

            @pl.when(k < z)
            def _():
                send(s2_send, s2_recv.at[k], m2s_sem.at[k], m2r_sem.at[k], {"sp_0": k}).wait_recv()
                b_k = joined_rows(s2_recv[k, pl.ds(DK, 16), :])
                run_v[...] = jnp.exp2(b_k) * run_v[...] + s2_recv[k, pl.ds(0, DK), :].astype(F32)

        run = run_v[...]
        for k in range(NX):
            s3_send[k] = (jnp.exp2(bsum_v[k][0:1, :]) * run + pre_v[k]).astype(BF16)

        for d in (2, 1, 3):
            msg3(d).start()

    row_at = jnp.where(x == 0, 1, 0)
    column_at = row_at + jnp.where(z == 0, 0, jnp.where((tp == 0) | (z == 2), 2, 1))

    def prefixes(at):
        if at <= 1:

            @pl.when(row_at == at)
            def _():
                row_prefix()

        @pl.when(column_at == at)
        def _():
            column_prefix()

    prefixes(0)

    first[4].wait()
    second[4].wait()
    for k in range(2, 7):
        params[k].wait()

    def gate_dots(c):
        g = dot(x_v[tile(c), :], wg_v[...])
        gain = jnp.concatenate([rgain_v[...]] * NH, axis=1)
        gate_v[tile(c), :] = silu(g) * gain

    pool_sends = [
        send(a_v.at[tile(c), pl.ds(0, C)], a_v.at[tile(c), pl.ds(C, C)], ps_sem.at[c], pr_sem.at[c], partner)
        for c in range(NT)
    ]

    def pooling(b):
        position = sp * T + b * B + lax.broadcasted_iota(jnp.int32, (B, 1), 0) + 1
        for g in range(2):
            cols = slice(g * 256, (g + 1) * 256)
            total = dot(band_v[g], pooled_v[pl.ds(b * B, 2 * B), cols])
            here = pooled_v[pl.ds((b + 1) * B, B), cols].astype(F32)
            width = jnp.left_shift(2, 2 * tp + g)
            if b == 0:
                diff = total / jnp.minimum(position, width).astype(F32) - here
            else:
                diff = total * (1.0 / width.astype(F32)) - here
            mixed = dot(diff.astype(BF16), pmix_v[g]) * pscale_v[:, cols]
            a_v[pl.ds(b * B, B), cols] = mixed.astype(BF16)

    def pool_tiles(c):
        for k in range(R // B):
            pooling(c * (R // B) + k)

    gate_dots(0)
    gate_dots(1)
    pool_tiles(1)
    pool_sends[1].start()

    prefixes(1)

    gate_dots(2)
    pool_tiles(2)
    pool_sends[2].start()

    prefixes(2)

    @pl.when(jnp.logical_not(is_first))
    def _():
        halo.wait_recv()
        pooled_v[pl.ds(B - 16, 16), :] = halo_v[...]

    gate_dots(3)
    pool_tiles(3)
    pool_tiles(0)
    pool_sends[3].start()
    pool_sends[0].start()
    prefixes(3)

    for c in out_loads:
        c.wait()
    for c in w_sends:
        c.wait_recv()
    def pool_project(c):
        resid_v[tile(c), :] = ALPHA * x_v[tile(c), 0:H].astype(F32) + dot(
            a_v[tile(c), 0 : 2 * C], wo_v[0 : 2 * C, :]
        )

    for c in range(1, NT):
        pool_sends[c].wait_recv()
        pool_project(c)

    s3_recv[x] = s3_send[x]
    for d in range(1, NX):
        arrival3(d).wait_recv()

    rec_sends = [
        send(
            a_v.at[tile(c), pl.ds(2 * C, C)], a_v.at[tile(c), pl.ds(3 * C, C)],
            rs_sem.at[c], rr_sem.at[c], partner,
        )
        for c in range(NT)
    ]
    stat_sends = [
        send(stat_v.at[tile(c), :], ostat_v.at[tile(c), :], ss_sem.at[c], sr_sem.at[c], partner)
        for c in range(NT)
    ]

    def recur(b):
        rows = pl.ds(b * B, B)
        far = jnp.exp2(off_v[b])
        for h in range(NH):
            hs = slice(h * DK, (h + 1) * DK)
            state = st_v[b, h] + far[:, hs] * s3_recv[h].astype(F32)
            raw = dot(sq_v[rows, 2 * h * DK : (2 * h + 1) * DK], v_v[rows, hs])
            raw = raw + dot_nt(sq_v[rows, (2 * h + 1) * DK : (2 * h + 2) * DK], state.astype(BF16))
            power = jnp.mean(raw * raw, axis=1, keepdims=True)
            normed = raw * lax.rsqrt(power + EPS_RMS) * gate_v[rows, hs]
            a_v[rows, 2 * C + h * DK : 2 * C + (h + 1) * DK] = normed.astype(BF16)

    def project(c):
        resid_v[tile(c), :] = resid_v[tile(c), :] + dot(
            a_v[tile(c), 2 * C : 4 * C], wo_v[2 * C : 4 * C, :]
        )

    def stats(c):
        resid = resid_v[tile(c), :]
        mean = jnp.sum(resid, axis=1, keepdims=True) * (1.0 / H)
        dev = resid - mean
        m2 = jnp.sum(dev * dev, axis=1, keepdims=True)
        lane = lax.broadcasted_iota(jnp.int32, (R, DK), 1)
        stat_v[tile(c), :] = jnp.where(lane == 0, mean, m2)

    def norm(c):
        mine = stat_v[tile(c), :]
        theirs = ostat_v[tile(c), :]
        gap = mine[:, 0:1] - theirs[:, 0:1]
        mean = 0.5 * (mine[:, 0:1] + theirs[:, 0:1])
        var = (mine[:, 1:2] + theirs[:, 1:2] + gap * gap * (0.5 * H)) * (1.0 / (2 * H))
        scale = lax.rsqrt(var + EPS_NORM)
        out[tile(c), :] = (
            (resid_v[tile(c), :] - mean) * scale * ngain_v[...] + nbias_v[...]
        ).astype(BF16)

    def recur_tile(c):
        for k in range(R // B):
            recur(c * (R // B) + k)
        rec_sends[c].start()

    recur_tile(0)
    pool_sends[0].wait_recv()
    for k in range(R // B, 3 * R // B):
        recur(k)
    pool_project(0)
    rec_sends[1].start()
    rec_sends[2].start()
    rec_sends[0].wait_recv()
    for k in range(3 * R // B, T // B):
        recur(k)
    project(0)
    rec_sends[3].start()
    for c in range(1, NT):
        rec_sends[c].wait_recv()
        project(c)
        stats(c - 1)
        stat_sends[c - 1].start()
    stats(NT - 1)
    stat_sends[NT - 1].start()
    for c in range(NT):
        stat_sends[c].wait_recv()
        norm(c)

    for c in range(NT):
        x_sends[c].wait_send()
        pool_sends[c].wait_send()
        rec_sends[c].wait_send()
        stat_sends[c].wait_send()
    for c in w_sends:
        c.wait_send()

    @pl.when(jnp.logical_not(is_last))
    def _():
        halo.wait_send()

    for d in range(1, NX):
        msg1(d).wait_send()
        msg3(d).wait_send()
    for k in range(1, nz):

        @pl.when(k > z)
        def _():
            msg2(k).wait_send()


def layer(nz, *args):
    (stream, wp, wq, wf, wv, wg, pmix, pscale, lb, ed, rgain, wop, wor, ngain, nbias) = args
    sem = pltpu.SemaphoreType.DMA
    scratch = [
        pltpu.VMEM((T, 2 * H), BF16),
        *[pltpu.VMEM((2 * H, C), BF16)] * 5,
        pltpu.VMEM((4 * C, H), BF16),
        pltpu.VMEM((2, 256, 256), BF16),
        pltpu.VMEM((1, C), F32),
        pltpu.VMEM((1, C), F32),
        pltpu.VMEM((NH, T), F32),
        pltpu.VMEM((T, NH), F32),
        pltpu.VMEM((1, DK), F32),
        pltpu.VMEM((1, H), F32),
        pltpu.VMEM((1, H), F32),
        pltpu.VMEM((T, C), F32),
        pltpu.VMEM((4, 2 * B, C), BF16),
        pltpu.VMEM((T, C), BF16),
        pltpu.VMEM((NB, 1, C), F32),
        pltpu.VMEM((T, C), BF16),
        pltpu.VMEM((T, C), F32),
        pltpu.VMEM((T, C), BF16),
        pltpu.VMEM((T + B, C), BF16),
        pltpu.VMEM((16, C), BF16),
        pltpu.VMEM((T, 2 * C), BF16),
        pltpu.VMEM((T, C), F32),
        pltpu.VMEM((T, 4 * C), BF16),
        pltpu.VMEM((NB, NH, DK, DK), F32),
        pltpu.VMEM((NH, DK, DK), F32),
        pltpu.VMEM((NB, 1, C), F32),
        pltpu.VMEM((1, C), F32),
        pltpu.VMEM((2, B, 2 * B), BF16),
        pltpu.VMEM((B, 2 * B), BF16),
        pltpu.VMEM((NH, MSG, DK), BF16),
        pltpu.VMEM((NX, MSG, DK), BF16),
        pltpu.VMEM((MSG, DK), BF16),
        pltpu.VMEM((nz, MSG, DK), BF16),
        pltpu.VMEM((NX, DK, DK), BF16),
        pltpu.VMEM((NX, DK, DK), BF16),
        pltpu.VMEM((NX, DK, DK), F32),
        pltpu.VMEM((NX, 8, DK), F32),
        pltpu.VMEM((DK, DK), F32),
        pltpu.VMEM((T, H), F32),
        pltpu.VMEM((T, DK), F32),
        pltpu.VMEM((T, DK), F32),
        sem((NT + 12,)), sem((7,)),
        sem((NT,)), sem((NT,)), sem((2,)), sem((2,)), sem((NT,)), sem((NT,)),
        sem((NT,)), sem((NT,)), sem((NT,)), sem((NT,)),
        sem, sem,
        sem((NX - 1,)), sem((NX,)), sem((nz,)), sem((nz,)), sem((NX - 1,)), sem((NX,)),
    ]
    operands = (
        stream[0], wp, wq, wf, wv, wg, pmix,
        pscale.reshape(1, C), lb.reshape(1, C), ed.T, rgain.reshape(1, DK),
        wop, wor, ngain.reshape(1, H), nbias.reshape(1, H),
    )
    result = pl.pallas_call(
        functools.partial(kernel, nz),
        out_shape=pltpu.VMEM((T, H), BF16),
        in_specs=[pl.BlockSpec(memory_space=pltpu.HBM)] * 15,
        out_specs=pl.BlockSpec(memory_space=pltpu.VMEM),
        scratch_shapes=scratch,
        compiler_params=pltpu.CompilerParams(
            collective_id=0, has_side_effects=True, vmem_limit_bytes=58_000_000
        ),
    )(*[pltpu.with_memory_space_constraint(a, pltpu.HBM) for a in operands])
    return result[None]


def solution(mesh):
    devices = mesh.devices
    nz = devices.shape[0] // NX
    torus = Mesh(
        devices.reshape(nz, NX, mesh.shape["fs"], mesh.shape["tp"]), ("sp_0", "sp_1", "fs", "tp")
    )
    sp = ("sp_0", "sp_1")
    cols = P(None, "tp")
    return jax.shard_map(
        functools.partial(layer, nz),
        mesh=torus,
        in_specs=(
            P("fs", sp, "tp"), cols, cols, cols, cols, cols,
            P("tp", None, None), P("tp"), P("tp"), P(sp, "tp"), P(),
            P("tp", None), P("tp", None), P("tp"), P("tp"),
        ),
        out_specs=P("fs", sp, "tp"),
        check_vma=False,
    )
```
